32 devices in a mesh: sp: 8 (over z, x), tp: 4 (over y, core).
Axes of the slice: x: 2, y: 2, z: 4, core: 2. Of those that a mesh axis runs over, the one named last changes fastest.
Arguments:
- query_matrix: bfloat16 [2048, 1024], P('sp', 'tp'), may hold values from -6 to 6
- key_matrix: bfloat16 [2048, 1024], P('sp', 'tp'), may hold values from -6 to 6
- value_matrix: bfloat16 [2048, 2048], P('sp', 'tp'), may hold values from -6 to 6
- output_gate_rows: bfloat16 [2048, 2048], P('sp', 'tp'), may hold values from -6 to 6
- decay_preactivation: bfloat16 [2048, 1024], P('sp', 'tp'), may hold values from -5 to 5
- channel_decay_bias: float32 [1024], P('tp'), may hold values from 0 to 10
- extra_log_decay: float32 [2048, 16], P('sp', 'tp'), may hold values from -0.7 to 0
- head_norm_gain: float32 [128], replicated, may hold values from 0.1 to 1.9
- output_projection: bfloat16 [2048, 2048], P('tp'), may hold values from -0.125 to 0.125
- residual_input: bfloat16 [2048, 2048], P(('sp', 'tp')), may hold values from -6 to 6
- attention_norm_gain: float32 [2048], replicated, may hold values from 0.1 to 1.9
- expert_before_gain: float32 [2048], replicated, may hold values from 0.1 to 1.9
- expert_after_gain: float32 [2048], replicated, may hold values from 0.1 to 1.9
- expert_gate_weight: bfloat16 [8, 2048, 4096], P('sp', None, 'tp'), may hold values from -0.125 to 0.125
- expert_up_weight: bfloat16 [8, 2048, 4096], P('sp', None, 'tp'), may hold values from -0.125 to 0.125
- expert_down_weight: bfloat16 [8, 4096, 2048], P('sp', 'tp'), may hold values from -0.09375 to 0.09375
- token_expert_index: int32 [2048, 2], P('sp'), may hold values from 0 to 7, as said below
- routing_weight_matrix: float32 [2048, 2], P('sp'), may hold values from 0.1 to 1
Outputs:
- layer_out: bfloat16 [2048, 2048], P(('sp', 'tp'))
The draws below stay inside these ranges and needn't reach their ends.
Inputs may be any that keep to these rules, and one draw needn't show every extreme that they name: `token_expert_index`: the 2 experts of a token differ and lie in one group: they have the same value of e // 4. In each aligned block of 256 rows (the rows of one index of sp) no expert is named by more than 80 rows, and the 4 experts of one group are each named by exactly 80 rows in every block.
All inputs are finite; a program needn't handle non-finite values.
Results may differ from the reference program's by a relative error of at most 0.024.
Values may be sent and summed in bfloat16 or wider, within the bound.
A program may use at most 64 MiB of HBM per device.

```python
import jax
import jax.numpy as jnp
from jax import lax

D = 2048
HEAD_TOTAL = 16
KEY_CHANNELS = 64
DV = 128
FF = 4096
GROUP_SIZE = 4
TOP = 2
BLOCK = 64
TOK_DEV = 256
SEQUENCE_TOKENS = 2048
KEYW = 1024
VALW = 2048
EXPERTS = 8
N_SP = 8
N_TP = 4


def draw_decay_preactivation(key, part):
    noise_key, shift_key = jax.random.split(jax.random.fold_in(key, 12))
    block_count = SEQUENCE_TOKENS // TOK_DEV
    noise = jnp.clip(jax.random.normal(noise_key, (block_count, TOK_DEV, KEYW), jnp.float32), -4.0, 4.0)
    shift = jax.random.uniform(shift_key, (block_count, 1, KEYW), jnp.float32, -1.0, 1.0)
    return (noise + shift).reshape(SEQUENCE_TOKENS, KEYW).astype(jnp.bfloat16)


def draw_channel_decay_bias(key, part):
    pick_key, fast_key, slow_key = jax.random.split(jax.random.fold_in(key, 11), 3)
    fast_share = 0.5
    fast_head = jax.random.uniform(pick_key, (HEAD_TOTAL, 1), jnp.float32) < fast_share
    fast_bias = jax.random.uniform(fast_key, (HEAD_TOTAL, KEY_CHANNELS), jnp.float32, 0.0, 1.0)
    slow_bias = jax.random.uniform(slow_key, (HEAD_TOTAL, KEY_CHANNELS), jnp.float32, 8.5, 10.0)
    return jnp.where(fast_head, fast_bias, slow_bias).reshape(HEAD_TOTAL * KEY_CHANNELS)


def draw_extra_log_decay(key, part):
    position_random_key, size_key = jax.random.split(jax.random.fold_in(key, 13))
    spike_positions = jax.random.randint(position_random_key, (3, HEAD_TOTAL), 0, SEQUENCE_TOKENS)
    kept_share = jax.random.uniform(size_key, (3, HEAD_TOTAL), jnp.float32, 0.5, 0.8)
    match_table = (jnp.arange(SEQUENCE_TOKENS)[:, None, None] == spike_positions[None]).astype(jnp.float32)
    return jnp.sum(match_table * jnp.log(kept_share)[None], axis=1)


def draw_token_expert_index(key, part):
    base_key = jax.random.fold_in(key, 14)
    group_count = N_SP // GROUP_SIZE
    capacity = 5 * TOK_DEV // (2 * N_SP)
    full_rows = 2 * capacity
    others = group_count - 1
    unit_count = (TOK_DEV - full_rows) // GROUP_SIZE
    full_group = jax.random.randint(jax.random.fold_in(base_key, 0), (), 0, group_count)
    mark_index = jnp.arange(others + 1, dtype=jnp.int32)
    marks_base = mark_index * unit_count // others
    interior = ((mark_index > 0) & (mark_index < others)).astype(jnp.int32)
    jitter = jax.random.randint(jax.random.fold_in(base_key, 1), (N_SP, others + 1), 0, 2) * interior[None, :]
    bounds = full_rows + GROUP_SIZE * (marks_base[None, :] + jitter)
    ranks = jnp.arange(TOK_DEV, dtype=jnp.int32)
    passed = jnp.sum((ranks[None, :, None] >= bounds[:, None, 1:others]).astype(jnp.int32), axis=2)
    group_start = jnp.take_along_axis(bounds, passed, axis=1)
    in_full = ranks[None, :] < full_rows
    local_rank = jnp.where(in_full, ranks[None, :], ranks[None, :] - group_start)
    group_id = jnp.where(in_full, full_group, passed + (passed >= full_group).astype(jnp.int32))
    offsets = jax.random.randint(jax.random.fold_in(base_key, 2), (N_SP, group_count), 0, GROUP_SIZE)
    strides = jax.random.randint(jax.random.fold_in(base_key, 3), (N_SP, group_count), 1, GROUP_SIZE)
    offset_row = jnp.take_along_axis(offsets, group_id, axis=1)
    stride_row = jnp.take_along_axis(strides, group_id, axis=1)
    first_expert = group_id * GROUP_SIZE + (local_rank + offset_row) % GROUP_SIZE
    second_expert = group_id * GROUP_SIZE + (local_rank + offset_row + stride_row) % GROUP_SIZE
    paired = jnp.stack([first_expert, second_expert], axis=-1)
    order_keys = jax.random.split(jax.random.fold_in(base_key, 4), N_SP)
    orders = jax.vmap(lambda order_key: jax.random.permutation(order_key, TOK_DEV))(order_keys)
    block_rows = jnp.arange(N_SP, dtype=jnp.int32)[:, None]
    placed = jnp.zeros_like(paired).at[block_rows, orders].set(paired)
    return placed.reshape(SEQUENCE_TOKENS, TOP).astype(jnp.int32)


def block_levels(rng, shape, shards, least, top_value):
    def one(axis_at, blocks):
        draws = jax.random.uniform(jax.random.fold_in(jax.random.fold_in(rng, 6), axis_at), (blocks,), jnp.float32, least / len(shards), top_value / len(shards))
        return jnp.repeat(jnp.exp(draws), shape[axis_at] // blocks).reshape((-1,) + (1,) * (len(shape) - axis_at - 1))

    loudness = one(*shards[0])
    for cut in shards[1:]:
        loudness = loudness * one(*cut)
    return loudness


def gaussian(key, extent, deviation, bound, cuts=(), kind=jnp.bfloat16):
    gain = block_levels(key, extent, cuts, -0.22, 0.18) if cuts else 1.0
    entries = jax.random.normal(key, extent, jnp.float32) * deviation * gain
    return jnp.minimum(jnp.maximum(entries, -bound), bound).astype(kind)


def setup_inputs(seed: int = 0) -> dict:
    streams_of = jax.random.split(jax.random.key(seed), 19)
    return {
        "query_matrix": gaussian(streams_of[0], (SEQUENCE_TOKENS, KEYW), 1.0, 6.0, ((0, 8), (1, 4))),
        "key_matrix": gaussian(streams_of[1], (SEQUENCE_TOKENS, KEYW), 1.0, 6.0, ((0, 8), (1, 4))),
        "value_matrix": gaussian(streams_of[2], (SEQUENCE_TOKENS, VALW), 1.0, 6.0, ((0, 8), (1, 4))),
        "output_gate_rows": gaussian(streams_of[3], (SEQUENCE_TOKENS, VALW), 1.0, 6.0, ((0, 8), (1, 4))),
        "decay_preactivation": draw_decay_preactivation(jax.random.fold_in(streams_of[18], 71), 0),
        "channel_decay_bias": draw_channel_decay_bias(jax.random.fold_in(streams_of[18], 71), 0),
        "extra_log_decay": draw_extra_log_decay(jax.random.fold_in(streams_of[18], 71), 0),
        "head_norm_gain": jnp.clip(1.0 + 0.18 * jax.random.normal(streams_of[7], (DV,), jnp.float32), 0.1, 1.9),
        "output_projection": gaussian(streams_of[8], (VALW, D), VALW ** -0.5, 0.125, ((0, 4),)),
        "residual_input": gaussian(streams_of[9], (SEQUENCE_TOKENS, D), 1.0, 6.0, ((0, 32),)),
        "attention_norm_gain": jnp.clip(1.0 + 0.18 * jax.random.normal(streams_of[10], (D,), jnp.float32), 0.1, 1.9),
        "expert_before_gain": jnp.clip(1.0 + 0.18 * jax.random.normal(streams_of[11], (D,), jnp.float32), 0.1, 1.9),
        "expert_after_gain": jnp.clip(1.0 + 0.18 * jax.random.normal(streams_of[12], (D,), jnp.float32), 0.1, 1.9),
        "expert_gate_weight": gaussian(streams_of[13], (EXPERTS, D, FF), D ** -0.5, 0.125, ((0, 8), (2, 4))),
        "expert_up_weight": gaussian(streams_of[14], (EXPERTS, D, FF), D ** -0.5, 0.125, ((0, 8), (2, 4))),
        "expert_down_weight": gaussian(streams_of[15], (EXPERTS, FF, D), FF ** -0.5, 0.09375, ((0, 8), (1, 4))),
        "token_expert_index": draw_token_expert_index(jax.random.fold_in(streams_of[18], 71), 0),
        "routing_weight_matrix": jnp.clip(0.1 + 0.9 * jax.random.uniform(streams_of[17], (SEQUENCE_TOKENS, TOP), jnp.float32) ** block_levels(streams_of[17], (SEQUENCE_TOKENS, TOP), ((0, 8),), -0.2, 0.2), 0.1, 1.0),
    }


EPSILON = 1e-06
DECAY_NORMALIZER = 16.0
HIGHEST = lax.Precision.HIGHEST

def rms_scale(values, gain_row):
    return values * lax.rsqrt(lax.optimization_barrier(jnp.mean(values * values, axis=-1, keepdims=True)) + EPSILON) * gain_row

def rounded(values):
    return lax.optimization_barrier(values.astype(jnp.bfloat16)).astype(jnp.float32)

def blockwise_state(queries, keys_all, values_all, decay_logarithm):
    sequence_length, number_heads, width_k = queries.shape
    width_v = values_all.shape[-1]
    blocks = sequence_length // BLOCK
    q_blocks = queries.reshape(blocks, BLOCK, number_heads, width_k)
    k_blocks = keys_all.reshape(blocks, BLOCK, number_heads, width_k)
    v_blocks = values_all.reshape(blocks, BLOCK, number_heads, width_v)
    inside = jnp.cumsum(decay_logarithm.reshape(blocks, BLOCK, number_heads, width_k), axis=1)
    block_end = inside[:, -1:]
    q_decayed = q_blocks * jnp.exp(inside)
    k_inverse = k_blocks * jnp.exp(-inside)
    k_to_end = k_blocks * jnp.exp(block_end - inside)
    causal = jnp.tril(jnp.ones((BLOCK, BLOCK), dtype=bool))
    scores = jnp.einsum('nihd,njhd->nhij', q_decayed, k_inverse, precision=HIGHEST)
    scores = jnp.where(causal, scores, 0.0)
    within = jnp.einsum('nhij,njhv->nihv', scores, v_blocks, precision=HIGHEST)
    growth = jnp.einsum('nchd,nchv->nhdv', k_to_end, v_blocks, precision=HIGHEST)
    fade_rows = jnp.exp(block_end[:, 0])

    def advance(running_state, inputs_pair):
        fade_now, grow_now = inputs_pair
        return (fade_now[..., None] * running_state + grow_now, running_state)
    zero_state = jnp.zeros((number_heads, width_k, width_v), jnp.float32)
    _, starts = lax.scan(advance, zero_state, (fade_rows, growth))
    across = jnp.einsum('nchd,nhdv->nchv', q_decayed, starts, precision=HIGHEST)
    return (within + across).reshape(sequence_length, number_heads, width_v)

def reference(query_matrix, key_matrix, value_matrix, output_gate_rows, decay_preactivation, channel_decay_bias, extra_log_decay, head_norm_gain, output_projection, residual_input, attention_norm_gain, expert_before_gain, expert_after_gain, expert_gate_weight, expert_up_weight, expert_down_weight, token_expert_index, routing_weight_matrix):
    sequence_length = query_matrix.shape[0]
    number_heads = value_matrix.shape[1] // DV
    model_width = residual_input.shape[1]
    queries = query_matrix.astype(jnp.float32).reshape(sequence_length, number_heads, KEY_CHANNELS) * KEY_CHANNELS ** (-0.5)
    keys_all = key_matrix.astype(jnp.float32).reshape(sequence_length, number_heads, KEY_CHANNELS)
    values_all = value_matrix.astype(jnp.float32).reshape(sequence_length, number_heads, DV)
    decay_logarithm = jax.nn.log_sigmoid(decay_preactivation.astype(jnp.float32) + channel_decay_bias) / DECAY_NORMALIZER
    decay_logarithm = decay_logarithm.reshape(sequence_length, number_heads, KEY_CHANNELS) + extra_log_decay[:, :, None]
    attn = blockwise_state(queries, keys_all, values_all, decay_logarithm)
    gate_act = jax.nn.silu(output_gate_rows.astype(jnp.float32).reshape(sequence_length, number_heads, DV))
    gated = (rms_scale(attn, head_norm_gain) * gate_act).astype(jnp.bfloat16)
    per_group = number_heads // N_TP
    grouped = gated.reshape(sequence_length, N_TP, per_group * DV).transpose(1, 0, 2)
    group_weights = output_projection.reshape(N_TP, per_group * DV, model_width)

    def add_group(total_sum, pair_in):
        group_rows, group_weight = pair_in
        return (total_sum + rounded(jnp.dot(group_rows, group_weight, preferred_element_type=jnp.float32)), None)
    mixed, _ = lax.scan(add_group, jnp.zeros((sequence_length, model_width), jnp.float32), (grouped, group_weights))
    layer_mid = (residual_input.astype(jnp.float32) + rms_scale(mixed, attention_norm_gain)).astype(jnp.bfloat16)
    normed = rms_scale(layer_mid.astype(jnp.float32), expert_before_gain).astype(jnp.bfloat16)
    expert_count = N_SP
    capacity = 5 * TOK_DEV // (2 * expert_count)
    block_ids = token_expert_index.reshape(N_SP, TOK_DEV * TOP)
    one_hot = (block_ids[:, :, None] == jnp.arange(expert_count, dtype=jnp.int32)[None, None, :]).astype(jnp.int32)
    slot_index = lax.optimization_barrier(jnp.sum((jnp.cumsum(one_hot, axis=1) - one_hot) * one_hot, axis=2))
    block_index = jnp.arange(N_SP, dtype=jnp.int32)[:, None]
    target = (block_ids * N_SP + block_index) * capacity + slot_index
    owners = jnp.zeros((expert_count * N_SP * capacity,), jnp.int32)
    owners = owners.at[target.reshape(-1)].set(jnp.arange(sequence_length * TOP, dtype=jnp.int32) // TOP)
    owners = owners.reshape(expert_count, N_SP * capacity)
    shard_width = FF // N_TP

    def run_expert(pack):
        row_index, w_gate, w_up, w_down = pack
        rows_in = normed[row_index]
        gate_part = jnp.dot(rows_in, w_gate, preferred_element_type=jnp.float32)
        up_part = jnp.dot(rows_in, w_up, preferred_element_type=jnp.float32)
        hidden = (jax.nn.silu(gate_part) * up_part).astype(jnp.bfloat16)
        hidden_parts = hidden.reshape(rows_in.shape[0], N_TP, shard_width).transpose(1, 0, 2)
        down_parts = w_down.reshape(N_TP, shard_width, model_width)

        def add_part(total_sum, pair_in):
            part_rows, part_weight = pair_in
            return (total_sum + rounded(jnp.dot(part_rows, part_weight, preferred_element_type=jnp.float32)), None)
        summed, _ = lax.scan(add_part, jnp.zeros((rows_in.shape[0], model_width), jnp.float32), (hidden_parts, down_parts))
        return summed.astype(jnp.bfloat16)
    served = lax.map(run_expert, (owners, expert_gate_weight, expert_up_weight, expert_down_weight))
    picked = served.reshape(-1, model_width)[target.reshape(sequence_length, TOP)].astype(jnp.float32)
    branch = lax.optimization_barrier(jnp.sum(routing_weight_matrix[:, :, None] * picked, axis=1))
    return (layer_mid.astype(jnp.float32) + rms_scale(branch, expert_after_gain)).astype(jnp.bfloat16)
```

```python
import contextlib
import functools

import jax
import jax.numpy as jnp
from jax import lax
from jax.experimental import pallas as pl
from jax.experimental.pallas import tpu as pltpu
from jax.sharding import PartitionSpec as P

KEY_CHANNELS = 64
DV = 128
TOP = 2
BLOCK = 64

EPSILON = 1e-06
DECAY_NORMALIZER = 16.0
HIGHEST = lax.Precision.HIGHEST
MESH = pl.DeviceIdType.MESH
F32 = jnp.float32
BF16 = jnp.bfloat16
FADE_ROWS = 16
PARTS = 4
TILE = 512
VMEM_LIMIT = 67043328


def scope(name):
    return contextlib.nullcontext()


def rms_scale(values, gain_row):
    return (
        values * lax.rsqrt(jnp.mean(values * values, axis=-1, keepdims=True) + EPSILON) * gain_row
    )


def contract(a, b, da, db):
    return lax.dot_general(a, b, (((da,), (db,)), ((), ())), preferred_element_type=F32)


def loop(count, body):
    def step(i, carry):
        body(i)
        return carry

    lax.fori_loop(0, count, step, 0)


def remote(src, dst, send, recv, device):
    return pltpu.make_async_remote_copy(
        src_ref=src,
        dst_ref=dst,
        send_sem=send,
        recv_sem=recv,
        device_id=device,
        device_id_type=MESH,
    )


def flipped(me, i, n):
    total, bit = 0, 1
    while bit < n:
        total = total + lax.rem(me // bit + i // bit, 2) * bit
        bit *= 2
    return total


def thirds(values):
    high = values.astype(BF16)
    rest = values - high.astype(F32)
    mid = rest.astype(BF16)
    return high, mid, (rest - mid.astype(F32)).astype(BF16)


def unit_order(n_sp):
    half = n_sp // 2
    pairs = [(i, 2) for i in range(0, half, 2)]
    singles = [(i, 1) for i in range(half, n_sp)]
    units = []
    while pairs or singles:
        if pairs:
            units.append(pairs.pop(0))
        if singles:
            units.append(singles.pop(0))
    return units


def layer_kernel(
    n_sp, n_tp, cap,
    d_hbm, bias_hbm, extra_hbm, k_hbm, v_hbm, q_hbm, g_hbm, hgain_hbm, index_hbm, weight_hbm,
    w_hbm, res_hbm, again_hbm, bgain_hbm, fgain_hbm, wg_hbm, wu_hbm, wd_hbm,
    out_ref,
    d_ref, bias_ref, extra_ref, k_ref, v_ref, q_ref, g_ref, hgain_ref, index_ref, weight_ref,
    w_ref, res_ref, again_ref, bgain_ref, fgain_ref, wg, wu, wd,
    message, pairbox, zmsg, inbox, carried, exch_out, exch_in, gated, part_ref, mixed_ref,
    ra, rb, tb, normed, xcol, sel_ref, mix_ref, outgoing, rows_ref, hidden, p_ref,
    r1, r2, ty, ob, back, acc, branch, brow, mid_ref,
    load, s_pair, r_pair, s_z, r_z,
    sa, va, sb, vb, st, vt, ss, vs, sy, vy, sd, vd, s1, v1, s2, v2, s3, v3, s4, v4,
):
    me = lax.axis_index("sp")
    j = lax.axis_index("tp")
    loads = [
        pltpu.make_async_copy(src, dst, load.at[n])
        for n, (src, dst) in enumerate(
            (
                (d_hbm, d_ref),
                (bias_hbm, bias_ref),
                (extra_hbm, extra_ref),
                (k_hbm, k_ref),
                (v_hbm, v_ref),
                (q_hbm, q_ref),
                (g_hbm, g_ref),
                (hgain_hbm, hgain_ref),
                (index_hbm, index_ref),
                (weight_hbm, weight_ref),
                (w_hbm, w_ref),
                (res_hbm, res_ref),
                (again_hbm, again_ref),
                (bgain_hbm, bgain_ref),
                (fgain_hbm, fgain_ref),
                (wg_hbm, wg),
                (wu_hbm, wu),
                (wd_hbm, wd),
            )
        )
    ]
    for copy in loads:
        copy.start()
    barrier = pltpu.get_barrier_semaphore()

    def along_sp(i):
        pl.semaphore_signal(
            barrier, inc=1, device_id={"sp": lax.rem(me + 1 + i, n_sp)}, device_id_type=MESH
        )

    def along_tp(i):
        pl.semaphore_signal(
            barrier, inc=1, device_id={"tp": lax.rem(j + 1 + i, n_tp)}, device_id_type=MESH
        )

    loop(n_sp - 1, along_sp)
    loop(n_tp - 1, along_tp)

    side = lax.rem(me, 2)
    pair = me // 2
    n_pair = n_sp // 2
    partner = me + 1 - 2 * side
    n_y = n_tp // 2
    y, c = j // 2, lax.rem(j, 2)
    sibling = 2 * y + 1 - c
    length, width = q_ref.shape
    rows, model = res_ref.shape
    share = model // n_tp
    half = n_sp // 2
    heads = width // KEY_CHANNELS
    blocks = length // BLOCK
    half_width = width // 2

    with scope("a_wait0"):
        for copy in loads[0:3]:
            copy.wait()
    with scope("a_decay"):
        x = d_ref[...].astype(F32) + bias_ref[...]
        log_decay = (jnp.minimum(x, 0.0) - jnp.log1p(jnp.exp(-jnp.abs(x)))) / DECAY_NORMALIZER
        row = lax.broadcasted_iota(jnp.int32, (length, length), 0)
        col = lax.broadcasted_iota(jnp.int32, (length, length), 1)
        causal = (row >= col) & (row // BLOCK == col // BLOCK)
        triangle = jnp.where(causal, 1.0, 0.0).astype(F32)
        ones = triangle.astype(BF16)
        inside = sum(jnp.dot(ones, p, preferred_element_type=F32) for p in thirds(log_decay))
        extra = lax.dot_general(
            triangle, extra_ref[...], (((1,), (1,)), ((), ())), precision=HIGHEST,
            preferred_element_type=F32,
        )
        inside = inside + jnp.concatenate(
            [jnp.broadcast_to(extra[:, h : h + 1], (length, KEY_CHANNELS)) for h in range(heads)],
            axis=1,
        )
    ends = [inside[(b + 1) * BLOCK - 1 : (b + 1) * BLOCK, :] for b in range(blocks)]
    offsets = [jnp.zeros_like(ends[0])]
    for b in range(blocks):
        offsets.append(offsets[-1] + ends[b])

    def spread(pieces):
        return jnp.concatenate([jnp.broadcast_to(r, (BLOCK, width)) for r in pieces], axis=0)

    for copy in loads[3:6]:
        copy.wait()
    with scope("a_state"):
        q = q_ref[...].astype(F32) * KEY_CHANNELS ** (-0.5)
        k = k_ref[...].astype(F32)
        k_end = (k * jnp.exp(spread(ends) - inside)).astype(BF16)
        states = [jnp.zeros((DV, width), F32)]
        for b in range(blocks):
            at = slice(b * BLOCK, (b + 1) * BLOCK)
            grown = jnp.concatenate(
                [
                    contract(
                        v_ref[at, h * DV : (h + 1) * DV],
                        k_end[at, h * KEY_CHANNELS : (h + 1) * KEY_CHANNELS],
                        0,
                        0,
                    )
                    for h in range(heads)
                ],
                axis=1,
            )
            states.append(states[-1] * jnp.exp(ends[b]) + grown)
        fade = jnp.exp(offsets[-1])
        for h in range(2):
            cs = slice(h * half_width, (h + 1) * half_width)
            message[h, 0:DV, :] = states[-1][:, cs].astype(BF16)
            message[h, DV:, :] = jnp.broadcast_to(fade[:, cs], (FADE_ROWS, half_width)).astype(BF16)

    with scope("a_barrier"):
        pl.semaphore_wait(barrier, n_sp + n_tp - 2)
    pair_copy = remote(
        message.at[1 - side], pairbox, s_pair.at[0], r_pair.at[0], {"sp": partner}
    )
    pair_copy.start()

    with scope("a_local"):
        q_in = (q * jnp.exp(inside)).astype(BF16)
        k_inv = (k * jnp.exp(-inside)).astype(BF16)
        q_all = (q * jnp.exp(inside + spread(offsets[:-1]))).astype(BF16)
        local = []
        for h in range(heads):
            cs = slice(h * KEY_CHANNELS, (h + 1) * KEY_CHANNELS)
            scores = jnp.where(causal, contract(q_in[:, cs], k_inv[:, cs], 1, 1), 0.0).astype(BF16)
            within = jnp.dot(scores, v_ref[:, h * DV : (h + 1) * DV], preferred_element_type=F32)
            across = jnp.concatenate(
                [jnp.zeros((BLOCK, DV), F32)]
                + [
                    contract(
                        q_in[b * BLOCK : (b + 1) * BLOCK, cs], states[b][:, cs].astype(BF16), 1, 1
                    )
                    for b in range(1, blocks)
                ],
                axis=0,
            )
            local.append(within + across)

    with scope("a_pair"):
        pair_copy.wait_recv()
        mine = message[side].astype(F32)
        other = pairbox[...].astype(F32)
        first = jnp.where(side == 0, mine, other)
        second = jnp.where(side == 0, other, mine)
        zmsg[0:DV, :] = (first[0:DV] * second[DV : DV + 1] + second[0:DV]).astype(BF16)
        zmsg[DV:, :] = (first[DV:] * second[DV:]).astype(BF16)

    def z_copy(i):
        return remote(
            zmsg, inbox.at[pair], s_z.at[i], r_z.at[pair],
            {"sp": 2 * jnp.minimum(pair + 1 + i, n_pair - 1) + side},
        )

    def z_send(i):
        @pl.when(pair + 1 + i < n_pair)
        def _():
            z_copy(i).start()

    loop(n_pair - 1, z_send)

    def peer_of(i):
        return flipped(me, i, n_sp)

    with scope("a_route"):
        loads[8].wait()
        loads[9].wait()
        e0, e1 = index_ref[0:1, :], index_ref[1:2, :]
        named = lax.broadcasted_iota(jnp.int32, (n_sp, length), 0)
        taken = jnp.where((named == e0) | (named == e1), 1.0, 0.0).astype(BF16)
        before = jnp.where(row < col, 1.0, 0.0).astype(BF16)
        counts = jnp.dot(taken, before, preferred_element_type=F32)

        def target(e):
            place = jnp.sum(jnp.where(named == e, counts, 0.0), axis=0, keepdims=True)
            return e.astype(F32) * cap + place

        t0, t1 = target(e0), target(e1)
        w0, w1 = weight_ref[0:1, :], weight_ref[1:2, :]

        def route(i):
            slot = lax.broadcasted_iota(jnp.int32, (cap, length), 0) + peer_of(i) * cap
            slot = slot.astype(F32)
            is0, is1 = slot == t0, slot == t1
            sel_ref[i] = jnp.where(is0 | is1, 1.0, 0.0).astype(BF16)
            mix_ref[i] = (jnp.where(is0, w0, 0.0) + jnp.where(is1, w1, 0.0)).astype(BF16)

        loop(n_sp, route)

    carried[...] = jnp.zeros_like(carried)

    def take(hop):
        @pl.when(hop < pair)
        def _():
            remote(
                zmsg, inbox.at[hop], s_z.at[0], r_z.at[hop], {"sp": partner}
            ).wait_recv()
            carried[...] = carried[...] * inbox[hop, DV : DV + 1, :].astype(F32) + inbox[
                hop, 0:DV, :
            ].astype(F32)

    with scope("a_take"):
        loop(n_pair - 1, take)

    with scope("a_exch"):
        before_pair = carried[...]
        head = jnp.where(
            side == 0, message[side].astype(F32), pairbox[...].astype(F32)
        )
        after_first = before_pair * head[DV : DV + 1] + head[0:DV]
        own_start = jnp.where(side == 0, before_pair, after_first)
        exch_out[...] = jnp.where(side == 0, after_first, before_pair).astype(BF16)
        exch_copy = remote(exch_out, exch_in, s_pair.at[1], r_pair.at[1], {"sp": partner})
        exch_copy.start()
        exch_copy.wait_recv()
        got = exch_in[...].astype(F32)
        start = jnp.concatenate(
            [jnp.where(side == 0, own_start, got), jnp.where(side == 0, got, own_start)], axis=1
        ).astype(BF16)

    for copy in loads[6:8]:
        copy.wait()
    with scope("a_gate"):
        for h in range(heads):
            cs = slice(h * KEY_CHANNELS, (h + 1) * KEY_CHANNELS)
            at = slice(h * DV, (h + 1) * DV)
            attn = local[h] + contract(q_all[:, cs], start[:, cs], 1, 1)
            gate = g_ref[:, at].astype(F32)
            gated[:, at] = (rms_scale(attn, hgain_ref[...]) * (gate * jax.nn.sigmoid(gate))).astype(
                BF16
            )

    def rows_of(index):
        return pl.ds(pl.multiple_of(index * rows, rows), rows)

    def cols_of(index):
        return pl.ds(pl.multiple_of(index * share, share), share)

    piece = model // PARTS

    def piece_of(q):
        return pl.ds(pl.multiple_of(q * piece, piece), piece)

    def y_at(i):
        return lax.rem(y + 1 + i, n_y)

    def y_from(i):
        return lax.rem(y + n_y - 1 - i, n_y)

    def head_pair(m, q):
        return remote(
            part_ref.at[rows_of(2 * y_at(m) + 1 - c), piece_of(q)], ra.at[m, :, piece_of(q)],
            sa.at[m, q], va.at[m, q], {"tp": sibling},
        )

    def head_far(m, q):
        return remote(
            tb.at[m, :, piece_of(q)], rb.at[m, :, piece_of(q)], sb.at[m, q], vb.at[m, q],
            {"tp": 2 * y_at(m) + c},
        )

    def project(t):
        m, q = t // PARTS, lax.rem(t, PARTS)
        at = pl.ds(pl.multiple_of(2 * y_at(m) * rows, 2 * rows), 2 * rows)
        part_ref[at, piece_of(q)] = jnp.dot(
            gated[at, :], w_ref[:, piece_of(q)], preferred_element_type=F32
        ).astype(BF16)
        head_pair(m, q).start()

    def pair_sum(t):
        m, q = t // PARTS, lax.rem(t, PARTS)
        head_pair(m, q).wait_recv()
        tb[m, :, piece_of(q)] = (
            part_ref[rows_of(2 * y_at(m) + c), piece_of(q)].astype(F32)
            + ra[m, :, piece_of(q)].astype(F32)
        ).astype(BF16)
        head_far(m, q).start()

    def whole_sum(q):
        head_pair(n_y - 1, q).wait_recv()
        total = part_ref[rows_of(j), piece_of(q)].astype(F32) + ra[
            n_y - 1, :, piece_of(q)
        ].astype(F32)
        for m in range(n_y - 1):
            head_far(m, q).wait_recv()
            total = total + rb[m, :, piece_of(q)].astype(F32)
        mixed_ref[:, piece_of(q)] = total

    with scope("e_proj"):
        loads[10].wait()
        loop(n_y * PARTS, project)
    with scope("e_pair"):
        loop((n_y - 1) * PARTS, pair_sum)
    with scope("e_rs"):
        loop(PARTS, whole_sum)
    with scope("e_norm"):
        for copy in loads[11:15]:
            copy.wait()
        mid = (res_ref[...].astype(F32) + rms_scale(mixed_ref[...], again_ref[...])).astype(BF16)
        mid_ref[...] = mid
        normed[...] = rms_scale(mid.astype(F32), bgain_ref[...]).astype(BF16)

    def turn_copy(i):
        peer = lax.rem(j + 1 + i, n_tp)
        return remote(
            normed.at[:, cols_of(peer)], xcol.at[rows_of(j)], st.at[i], vt.at[i], {"tp": peer}
        )

    with scope("e_turn"):
        loop(n_tp - 1, lambda i: turn_copy(i).start())
        xcol[rows_of(j), :] = normed[:, cols_of(j)]
        loop(n_tp - 1, lambda i: turn_copy(i).wait_recv())

    def picked(i):
        return jnp.dot(sel_ref[i], xcol[...], preferred_element_type=F32).astype(BF16)

    def out_copy(i):
        return remote(
            outgoing.at[i], rows_ref.at[i, :, cols_of(j)], ss.at[i], vs.at[i],
            {"sp": peer_of(i)},
        )

    def y_copy(i, m):
        place = rows_ref.at[i, :, cols_of(j)]
        return remote(place, place, sy.at[m, i], vy.at[m, i], {"tp": 2 * y_at(m) + c})

    def pair_forward(i, m, owner):
        place = rows_ref.at[i, :, cols_of(owner)]
        return remote(place, place, sd.at[m, i], vd.at[m, i], {"tp": sibling})

    def forward(i):
        for m in range(n_y - 1):
            y_copy(i, m).start()
        pair_forward(i, n_y - 1, j).start()

    def arrived(i):
        out_copy(i).wait_recv()
        forward(i)

    def relay(i):
        for m in range(n_y - 1):
            y_copy(i, m).wait_recv()
            pair_forward(i, m, 2 * y_from(m) + c).start()

    def ready(i):
        for m in range(n_y - 1):
            pair_forward(i, m, 2 * y_from(m) + c).wait_recv()
        pair_forward(i, n_y - 1, j).wait_recv()

    def part_pair(i, m):
        return remote(
            p_ref.at[i, :, cols_of(2 * y_at(m) + 1 - c)], r1.at[i, m],
            s1.at[i, m], v1.at[i, m], {"tp": sibling},
        )

    def part_far(i, m):
        return remote(
            ty.at[i, m], r2.at[i, m], s2.at[i, m], v2.at[i, m], {"tp": 2 * y_at(m) + c}
        )

    def back_copy(i):
        return remote(ob.at[i], back.at[i], s3.at[i], v3.at[i], {"sp": peer_of(i)})

    def pass_along(i):
        for m in range(n_y - 1):
            part_pair(i, m).wait_recv()
            ty[i, m] = (
                p_ref[i, :, cols_of(2 * y_at(m) + c)].astype(F32) + r1[i, m].astype(F32)
            ).astype(BF16)
            part_far(i, m).start()

    def summed(i):
        part_pair(i, n_y - 1).wait_recv()
        total = p_ref[i, :, cols_of(j)].astype(F32) + r1[i, n_y - 1].astype(F32)
        for m in range(n_y - 1):
            part_far(i, m).wait_recv()
            total = total + r2[i, m].astype(F32)
        return total.astype(BF16)

    def give_back(i):
        if i == 0:
            back[0] = summed(0)
        else:
            ob[i] = summed(i)
            back_copy(i).start()

    tile = min(TILE, wg.shape[1])
    steps = wg.shape[1] // tile

    def run_expert(first, count, after_first_up, after_up, after_first_down):
        batch = count * cap

        def up(t):
            cols = pl.ds(pl.multiple_of(t * tile, tile), tile)
            fed = rows_ref[first : first + count].reshape(batch, model)
            gate = jnp.dot(fed, wg[:, cols], preferred_element_type=F32)
            rise = jnp.dot(fed, wu[:, cols], preferred_element_type=F32)
            hidden[0:batch, cols] = (gate * jax.nn.sigmoid(gate) * rise).astype(BF16)

            @pl.when(t == 0)
            def _():
                after_first_up()

        loop(steps, up)
        after_up()

        def down(owner):
            made = jnp.dot(hidden[0:batch, :], wd[:, cols_of(owner)], preferred_element_type=F32)
            p_ref[first : first + count, :, cols_of(owner)] = made.astype(BF16).reshape(
                count, cap, share
            )

        def down_pair(m):
            down(2 * y_at(m) + 1 - c)
            for i in range(count):
                part_pair(first + i, m).start()
            down(2 * y_at(m) + c)

            @pl.when(m == 0)
            def _():
                after_first_down()

        loop(n_y, down_pair)

    units = unit_order(n_sp)
    total_units = len(units)

    def each(k, body):
        if 0 <= k < total_units:
            for i in range(units[k][0], units[k][0] + units[k][1]):
                body(i)

    def arrive(k):
        each(k, lambda i: arrived(i) if i > 0 else None)

    with scope("e_send"):
        rows_ref[0, :, cols_of(j)] = picked(0)
        forward(0)

        def send(t):
            i = jnp.where(lax.rem(t, 2) == 0, half + t // 2, 1 + t // 2)
            outgoing[i] = picked(i)
            out_copy(i).start()

        loop(n_sp - 1, send)
    with scope("e_arrive"):
        arrive(0)
        relay(0)
        arrive(1)
        arrive(2)
    with scope("e_relay"):
        for i in range(1, units[0][1]):
            relay(i)
    with scope("e_weights"):
        for copy in loads[15:]:
            copy.wait()
    for k, (first, count) in enumerate(units):
        with scope(f"e_ready{k}"):
            each(k, ready)
        with scope(f"e_run{k}"):
            run_expert(
                first,
                count,
                lambda: each(k - 1, pass_along),
                lambda: each(k + 1, relay),
                lambda: each(k - 2, give_back),
            )
        with scope(f"e_arrive{k}"):
            arrive(k + 3)
    with scope("e_give"):
        each(total_units - 1, pass_along)
        each(total_units - 2, give_back)
        each(total_units - 1, give_back)

    def weighed(i):
        return contract(mix_ref[i], back[i], 0, 0)

    with scope("e_gather"):
        acc[...] = weighed(0)

        def gather(t):
            back_copy(t + 1).wait_recv()
            acc[...] = acc[...] + weighed(t + 1)

        loop(n_sp - 2, gather)
        back_copy(n_sp - 1).wait_recv()
        branch[...] = (acc[...] + weighed(n_sp - 1)).astype(BF16)

    def home_copy(i):
        peer = lax.rem(j + 1 + i, n_tp)
        return remote(
            branch.at[rows_of(peer)], brow.at[:, cols_of(j)], s4.at[i], v4.at[i], {"tp": peer}
        )

    with scope("e_home"):
        loop(n_tp - 1, lambda i: home_copy(i).start())
        brow[:, cols_of(j)] = branch[rows_of(j), :]
        loop(n_tp - 1, lambda i: home_copy(i).wait_recv())
    with scope("e_out"):
        out_ref[...] = (
            mid_ref[...].astype(F32) + rms_scale(brow[...].astype(F32), fgain_ref[...])
        ).astype(BF16)

    with scope("e_drain"):
        pair_copy.wait_send()
        exch_copy.wait_send()

        def drain_z(i):
            @pl.when(pair + 1 + i < n_pair)
            def _():
                z_copy(i).wait_send()

        loop(n_pair - 1, drain_z)
        loop(n_y * PARTS, lambda t: head_pair(t // PARTS, lax.rem(t, PARTS)).wait_send())
        loop((n_y - 1) * PARTS, lambda t: head_far(t // PARTS, lax.rem(t, PARTS)).wait_send())

        def drain_sp(i):
            out_copy(i + 1).wait_send()
            back_copy(i + 1).wait_send()

        loop(n_sp - 1, drain_sp)

        def drain_turns(i):
            turn_copy(i).wait_send()
            home_copy(i).wait_send()

        loop(n_tp - 1, drain_turns)

        def drain(i):
            for m in range(n_y - 1):
                y_copy(i, m).wait_send()
                pair_forward(i, m, 2 * y_from(m) + c).wait_send()
                part_far(i, m).wait_send()
            pair_forward(i, n_y - 1, j).wait_send()
            for m in range(n_y):
                part_pair(i, m).wait_send()

        loop(n_sp, drain)


def dmas(*shapes):
    return [pltpu.SemaphoreType.DMA(s) for s in shapes]


def shards(
    n_sp,
    n_tp,
    query_matrix,
    key_matrix,
    value_matrix,
    output_gate_rows,
    decay_preactivation,
    channel_decay_bias,
    extra_log_decay,
    head_norm_gain,
    output_projection,
    residual_input,
    attention_norm_gain,
    expert_before_gain,
    expert_after_gain,
    expert_gate_weight,
    expert_up_weight,
    expert_down_weight,
    token_expert_index,
    routing_weight_matrix,
):
    length, width = query_matrix.shape
    model = output_projection.shape[1]
    rows = residual_input.shape[0]
    share = model // n_tp
    n_y = n_tp // 2
    capacity = 5 * length // (2 * n_sp)
    cap = (capacity + 15) // 16 * 16
    values = value_matrix.shape[1]
    hidden_units = expert_gate_weight.shape[2]
    by_peer = (n_sp, n_y)
    state = (DV + FADE_ROWS, width // 2)

    operands = (
        decay_preactivation,
        channel_decay_bias.reshape(1, width),
        extra_log_decay.T,
        key_matrix,
        value_matrix,
        query_matrix,
        output_gate_rows,
        head_norm_gain.reshape(1, DV),
        token_expert_index.T,
        routing_weight_matrix.T,
        output_projection,
        residual_input,
        attention_norm_gain.reshape(1, model),
        expert_before_gain.reshape(1, model),
        expert_after_gain.reshape(1, model),
        expert_gate_weight[0],
        expert_up_weight[0],
        expert_down_weight[0],
    )
    kept = [pltpu.VMEM(a.shape, a.dtype) for a in operands]
    return pl.pallas_call(
        functools.partial(layer_kernel, n_sp, n_tp, cap),
        out_shape=jax.ShapeDtypeStruct((rows, model), BF16),
        in_specs=[pl.BlockSpec(memory_space=pl.ANY)] * len(operands),
        out_specs=pl.BlockSpec(memory_space=pltpu.VMEM),
        scratch_shapes=kept
        + [
            pltpu.VMEM((2,) + state, BF16),
            pltpu.VMEM(state, BF16),
            pltpu.VMEM(state, BF16),
            pltpu.VMEM((n_sp // 2,) + state, BF16),
            pltpu.VMEM((DV, width // 2), F32),
            pltpu.VMEM((DV, width // 2), BF16),
            pltpu.VMEM((DV, width // 2), BF16),
            pltpu.VMEM((length, values), BF16),
            pltpu.VMEM((length, model), BF16),
            pltpu.VMEM((rows, model), F32),
            pltpu.VMEM((n_y, rows, model), BF16),
            pltpu.VMEM((n_y, rows, model), BF16),
            pltpu.VMEM((n_y, rows, model), BF16),
            pltpu.VMEM((rows, model), BF16),
            pltpu.VMEM((length, share), BF16),
            pltpu.VMEM((n_sp, cap, length), BF16),
            pltpu.VMEM((n_sp, cap, length), BF16),
            pltpu.VMEM((n_sp, cap, share), BF16),
            pltpu.VMEM((n_sp, cap, model), BF16),
            pltpu.VMEM((2 * cap, hidden_units), BF16),
            pltpu.VMEM((n_sp, cap, model), BF16),
            pltpu.VMEM(by_peer + (cap, share), BF16),
            pltpu.VMEM(by_peer + (cap, share), BF16),
            pltpu.VMEM(by_peer + (cap, share), BF16),
            pltpu.VMEM((n_sp, cap, share), BF16),
            pltpu.VMEM((n_sp, cap, share), BF16),
            pltpu.VMEM((length, share), F32),
            pltpu.VMEM((length, share), BF16),
            pltpu.VMEM((rows, model), BF16),
            pltpu.VMEM((rows, model), BF16),
        ]
        + dmas(
            (len(operands),), (2,), (2,), (n_sp // 2,), (n_sp // 2,),
            (n_y, PARTS), (n_y, PARTS), (n_y, PARTS), (n_y, PARTS),
            (n_tp,), (n_tp,), (n_sp,), (n_sp,),
            (n_y, n_sp), (n_y, n_sp), (n_y, n_sp), (n_y, n_sp),
            by_peer, by_peer, by_peer, by_peer, (n_sp,), (n_sp,), (n_tp,), (n_tp,),
        ),
        compiler_params=pltpu.CompilerParams(
            collective_id=1, has_side_effects=True, vmem_limit_bytes=VMEM_LIMIT
        ),
    )(*operands)


def solution(mesh):
    placed = (
        P("sp", "tp"),
        P("sp", "tp"),
        P("sp", "tp"),
        P("sp", "tp"),
        P("sp", "tp"),
        P("tp"),
        P("sp", "tp"),
        P(),
        P("tp", None),
        P(("sp", "tp"), None),
        P(),
        P(),
        P(),
        P("sp", None, "tp"),
        P("sp", None, "tp"),
        P("sp", "tp", None),
        P("sp", None),
        P("sp", None),
    )
    return jax.shard_map(
        functools.partial(shards, mesh.shape["sp"], mesh.shape["tp"]),
        mesh=mesh,
        in_specs=placed,
        out_specs=P(("sp", "tp"), None),
        check_vma=False,
    )
```

```python
import contextlib
import functools

import jax
import jax.numpy as jnp
from jax import lax
from jax.experimental import pallas as pl
from jax.experimental.pallas import tpu as pltpu
from jax.sharding import PartitionSpec as P

KEY_CHANNELS = 64
DV = 128
TOP = 2
BLOCK = 64

EPSILON = 1e-06
DECAY_NORMALIZER = 16.0
HIGHEST = lax.Precision.HIGHEST
MESH = pl.DeviceIdType.MESH
F32 = jnp.float32
BF16 = jnp.bfloat16
FADE_ROWS = 16
PARTS = 4
TILE = 512
VMEM_LIMIT = 67043328


def scope(name):
    return contextlib.nullcontext()


def rms_scale(values, gain_row):
    return (
        values * lax.rsqrt(jnp.mean(values * values, axis=-1, keepdims=True) + EPSILON) * gain_row
    )


def contract(a, b, da, db):
    return lax.dot_general(a, b, (((da,), (db,)), ((), ())), preferred_element_type=F32)


def loop(count, body):
    def step(i, carry):
        body(i)
        return carry

    lax.fori_loop(0, count, step, 0)


def remote(src, dst, send, recv, device):
    return pltpu.make_async_remote_copy(
        src_ref=src,
        dst_ref=dst,
        send_sem=send,
        recv_sem=recv,
        device_id=device,
        device_id_type=MESH,
    )


def flipped(me, i, n):
    total, bit = 0, 1
    while bit < n:
        total = total + lax.rem(me // bit + i // bit, 2) * bit
        bit *= 2
    return total


def thirds(values):
    high = values.astype(BF16)
    rest = values - high.astype(F32)
    mid = rest.astype(BF16)
    return high, mid, (rest - mid.astype(F32)).astype(BF16)


def schedule(far, spare):
    hooks = {}
    start = 0
    near = list(range(3, 3 + spare))
    units = [1, 2] + list(range(3 + spare, 1 + spare + far))
    end = 1 + spare + far

    def put(k, slot, name, unit):
        hooks.setdefault((k, slot), []).append((name, unit))

    put(start, "first", "arr", units[1])
    put(start, "up", "relay", units[0])
    put(units[0], "up", "relay", units[1])
    put(units[0], "down", "arr", units[2])
    put(units[1], "first", "pass", units[0])
    put(units[1], "up", "arr", units[3])
    for k in near:
        put(k - 1, "up", "relay", k)
    put(near[0], "first", "pass", units[1])
    put(near[0], "first", "pass", start)
    put(near[-1], "up", "relay", units[2])
    put(near[-1], "down", "give", units[0])
    for t in range(2, far):
        if t > 2:
            put(units[t], "first", "give", units[t - 2])
            put(units[t], "first", "pass", units[t - 1])
        if t + 1 < far:
            put(units[t], "up", "relay", units[t + 1])
        if t + 2 < far:
            put(units[t], "down", "arr", units[t + 2])
    put(end, "first", "pass", units[-1])
    for k in near:
        put(end, "first", "pass", k)
    put(end, "first", "give", units[-2])
    put(end, "first", "give", start)
    put(end, "first", "give", units[-1])
    for k in near:
        put(end, "first", "give", k)
    return hooks


def layer_kernel(
    n_sp, n_tp, cap,
    d_hbm, bias_hbm, extra_hbm, k_hbm, v_hbm, q_hbm, g_hbm, hgain_hbm, index_hbm, weight_hbm,
    w_hbm, res_hbm, again_hbm, bgain_hbm, fgain_hbm, wg_hbm, wu_hbm, wd_hbm,
    out_ref,
    d_ref, bias_ref, extra_ref, k_ref, v_ref, q_ref, g_ref, hgain_ref, index_ref, weight_ref,
    w_ref, res_ref, again_ref, bgain_ref, fgain_ref, wg, wu, wd,
    message, pairbox, zmsg, inbox, carried, exch_out, exch_in, gated, part_ref, mixed_ref,
    ra, rb, tb, normed, xcol, sel_ref, mix_ref, outgoing, rows_ref, hidden, p_ref,
    r1, r2, ty, ob, back, acc, branch, brow, mid_ref,
    load, s_pair, r_pair, s_z, r_z,
    sa, va, vn, sb, vb, st, vt, ss, vs, sy, vy, sd, vd, s1, v1, s2, v2, s3, v3, s4, v4,
):
    me = lax.axis_index("sp")
    j = lax.axis_index("tp")
    loads = [
        pltpu.make_async_copy(src, dst, load.at[n])
        for n, (src, dst) in enumerate(
            (
                (d_hbm, d_ref),
                (bias_hbm, bias_ref),
                (extra_hbm, extra_ref),
                (k_hbm, k_ref),
                (v_hbm, v_ref),
                (q_hbm, q_ref),
                (g_hbm, g_ref),
                (hgain_hbm, hgain_ref),
                (index_hbm, index_ref),
                (weight_hbm, weight_ref),
                (w_hbm, w_ref),
                (res_hbm, res_ref),
                (again_hbm, again_ref),
                (bgain_hbm, bgain_ref),
                (fgain_hbm, fgain_ref),
                (wg_hbm, wg),
                (wu_hbm, wu),
                (wd_hbm, wd),
            )
        )
    ]
    for copy in loads:
        copy.start()
    barrier = pltpu.get_barrier_semaphore()

    def along_sp(i):
        pl.semaphore_signal(
            barrier, inc=1, device_id={"sp": lax.rem(me + 1 + i, n_sp)}, device_id_type=MESH
        )

    def along_tp(i):
        pl.semaphore_signal(
            barrier, inc=1, device_id={"tp": lax.rem(j + 1 + i, n_tp)}, device_id_type=MESH
        )

    loop(n_sp - 1, along_sp)
    loop(n_tp - 1, along_tp)

    side = lax.rem(me, 2)
    pair = me // 2
    n_pair = n_sp // 2
    partner = me + 1 - 2 * side
    n_y = n_tp // 2
    y, c = j // 2, lax.rem(j, 2)
    sibling = 2 * y + 1 - c
    length, width = q_ref.shape
    rows, model = res_ref.shape
    share = model // n_tp
    half = n_sp // 2
    heads = width // KEY_CHANNELS
    blocks = length // BLOCK
    half_width = width // 2

    with scope("a_wait0"):
        for copy in loads[0:3]:
            copy.wait()
    with scope("a_decay"):
        x = d_ref[...].astype(F32) + bias_ref[...]
        log_decay = (jnp.minimum(x, 0.0) - jnp.log1p(jnp.exp(-jnp.abs(x)))) / DECAY_NORMALIZER
        row = lax.broadcasted_iota(jnp.int32, (length, length), 0)
        col = lax.broadcasted_iota(jnp.int32, (length, length), 1)
        causal = (row >= col) & (row // BLOCK == col // BLOCK)
        triangle = jnp.where(causal, 1.0, 0.0).astype(F32)
        ones = triangle.astype(BF16)
        inside = sum(jnp.dot(ones, p, preferred_element_type=F32) for p in thirds(log_decay))
        extra = lax.dot_general(
            triangle, extra_ref[...], (((1,), (1,)), ((), ())), precision=HIGHEST,
            preferred_element_type=F32,
        )
        inside = inside + jnp.concatenate(
            [jnp.broadcast_to(extra[:, h : h + 1], (length, KEY_CHANNELS)) for h in range(heads)],
            axis=1,
        )
    ends = [inside[(b + 1) * BLOCK - 1 : (b + 1) * BLOCK, :] for b in range(blocks)]
    offsets = [jnp.zeros_like(ends[0])]
    for b in range(blocks):
        offsets.append(offsets[-1] + ends[b])

    def spread(pieces):
        return jnp.concatenate([jnp.broadcast_to(r, (BLOCK, width)) for r in pieces], axis=0)

    for copy in loads[3:6]:
        copy.wait()
    with scope("a_state"):
        q = q_ref[...].astype(F32) * KEY_CHANNELS ** (-0.5)
        k = k_ref[...].astype(F32)
        k_end = (k * jnp.exp(spread(ends) - inside)).astype(BF16)
        states = [jnp.zeros((DV, width), F32)]
        for b in range(blocks):
            at = slice(b * BLOCK, (b + 1) * BLOCK)
            grown = jnp.concatenate(
                [
                    contract(
                        v_ref[at, h * DV : (h + 1) * DV],
                        k_end[at, h * KEY_CHANNELS : (h + 1) * KEY_CHANNELS],
                        0,
                        0,
                    )
                    for h in range(heads)
                ],
                axis=1,
            )
            states.append(states[-1] * jnp.exp(ends[b]) + grown)
        fade = jnp.exp(offsets[-1])
        for h in range(2):
            cs = slice(h * half_width, (h + 1) * half_width)
            message[h, 0:DV, :] = states[-1][:, cs].astype(BF16)
            message[h, DV:, :] = jnp.broadcast_to(fade[:, cs], (FADE_ROWS, half_width)).astype(BF16)

    with scope("a_barrier"):
        pl.semaphore_wait(barrier, n_sp + n_tp - 2)
    pair_copy = remote(
        message.at[1 - side], pairbox, s_pair.at[0], r_pair.at[0], {"sp": partner}
    )
    pair_copy.start()

    with scope("a_local"):
        q_in = (q * jnp.exp(inside)).astype(BF16)
        k_inv = (k * jnp.exp(-inside)).astype(BF16)
        q_all = (q * jnp.exp(inside + spread(offsets[:-1]))).astype(BF16)
        local = []
        for h in range(heads):
            cs = slice(h * KEY_CHANNELS, (h + 1) * KEY_CHANNELS)
            scores = jnp.where(causal, contract(q_in[:, cs], k_inv[:, cs], 1, 1), 0.0).astype(BF16)
            within = jnp.dot(scores, v_ref[:, h * DV : (h + 1) * DV], preferred_element_type=F32)
            across = jnp.concatenate(
                [jnp.zeros((BLOCK, DV), F32)]
                + [
                    contract(
                        q_in[b * BLOCK : (b + 1) * BLOCK, cs], states[b][:, cs].astype(BF16), 1, 1
                    )
                    for b in range(1, blocks)
                ],
                axis=0,
            )
            local.append(within + across)

    def peer_of(i):
        return flipped(me, i, n_sp)

    with scope("a_route"):
        loads[8].wait()
        loads[9].wait()
        e0, e1 = index_ref[0:1, :], index_ref[1:2, :]
        named = lax.broadcasted_iota(jnp.int32, (n_sp, length), 0)
        taken = jnp.where((named == e0) | (named == e1), 1.0, 0.0).astype(BF16)
        before = jnp.where(row < col, 1.0, 0.0).astype(BF16)
        counts = jnp.dot(taken, before, preferred_element_type=F32)

        def target(e):
            place = jnp.sum(jnp.where(named == e, counts, 0.0), axis=0, keepdims=True)
            return e.astype(F32) * cap + place

        t0, t1 = target(e0), target(e1)
        w0, w1 = weight_ref[0:1, :], weight_ref[1:2, :]

        def route(i):
            slot = lax.broadcasted_iota(jnp.int32, (cap, length), 0) + peer_of(i) * cap
            slot = slot.astype(F32)
            is0, is1 = slot == t0, slot == t1
            sel_ref[i] = jnp.where(is0 | is1, 1.0, 0.0).astype(BF16)
            mix_ref[i] = (jnp.where(is0, w0, 0.0) + jnp.where(is1, w1, 0.0)).astype(BF16)

        loop(n_sp, route)

    with scope("a_pair"):
        pair_copy.wait_recv()
        mine = message[side].astype(F32)
        other = pairbox[...].astype(F32)
        first = jnp.where(side == 0, mine, other)
        second = jnp.where(side == 0, other, mine)
        zmsg[0:DV, :] = (first[0:DV] * second[DV : DV + 1] + second[0:DV]).astype(BF16)
        zmsg[DV:, :] = (first[DV:] * second[DV:]).astype(BF16)

    def z_copy(i):
        return remote(
            zmsg, inbox.at[pair], s_z.at[i], r_z.at[pair],
            {"sp": 2 * (n_pair - 1 - i) + side},
        )

    def z_send(i):
        @pl.when(n_pair - 1 - i > pair)
        def _():
            z_copy(i).start()

    loop(n_pair - 1, z_send)

    carried[...] = jnp.zeros_like(carried)

    def take(hop):
        @pl.when(hop < pair)
        def _():
            remote(
                zmsg, inbox.at[hop], s_z.at[0], r_z.at[hop], {"sp": partner}
            ).wait_recv()
            carried[...] = carried[...] * inbox[hop, DV : DV + 1, :].astype(F32) + inbox[
                hop, 0:DV, :
            ].astype(F32)

    with scope("a_take"):
        loop(n_pair - 1, take)

    with scope("a_exch"):
        before_pair = carried[...]
        head = jnp.where(
            side == 0, message[side].astype(F32), pairbox[...].astype(F32)
        )
        after_first = before_pair * head[DV : DV + 1] + head[0:DV]
        own_start = jnp.where(side == 0, before_pair, after_first)
        exch_out[...] = jnp.where(side == 0, after_first, before_pair).astype(BF16)
        exch_copy = remote(exch_out, exch_in, s_pair.at[1], r_pair.at[1], {"sp": partner})
        exch_copy.start()
        exch_copy.wait_recv()
        got = exch_in[...].astype(F32)
        start = jnp.concatenate(
            [jnp.where(side == 0, own_start, got), jnp.where(side == 0, got, own_start)], axis=1
        ).astype(BF16)

    for copy in loads[6:8]:
        copy.wait()
    with scope("a_gate"):
        for h in range(heads):
            cs = slice(h * KEY_CHANNELS, (h + 1) * KEY_CHANNELS)
            at = slice(h * DV, (h + 1) * DV)
            attn = local[h] + contract(q_all[:, cs], start[:, cs], 1, 1)
            gate = g_ref[:, at].astype(F32)
            gated[:, at] = (rms_scale(attn, hgain_ref[...]) * (gate * jax.nn.sigmoid(gate))).astype(
                BF16
            )

    def landed(ref, sem):
        remote(ref, ref, sem, sem, {"sp": partner}).wait_recv()

    def left(ref, sem):
        remote(ref, ref, sem, sem, {"sp": partner}).wait_send()

    def rows_of(index):
        return pl.ds(pl.multiple_of(index * rows, rows), rows)

    def cols_of(index):
        return pl.ds(pl.multiple_of(index * share, share), share)

    piece = model // PARTS

    def piece_of(q):
        return pl.ds(pl.multiple_of(q * piece, piece), piece)

    def y_at(i):
        return lax.rem(y + 1 + i, n_y)

    def y_from(i):
        return lax.rem(y + n_y - 1 - i, n_y)

    cuts = 2 if rows % 32 == 0 else 1
    band = rows // cuts

    def band_of(index, r):
        return pl.ds(pl.multiple_of(index * rows + r * band, band), band)

    def head_pair(m, r, q):
        return remote(
            part_ref.at[band_of(2 * y_at(m) + 1 - c, r), piece_of(q)],
            ra.at[m, band_of(0, r), piece_of(q)],
            sa, va.at[m, r, q], {"tp": sibling},
        )

    def head_near(r):
        return remote(
            part_ref.at[band_of(sibling, r)], ra.at[n_y - 1, band_of(0, r)], sa, vn.at[r],
            {"tp": sibling},
        )

    def head_far(m, r, q):
        return remote(
            tb.at[m, band_of(0, r), piece_of(q)], rb.at[m, band_of(0, r), piece_of(q)],
            sb, vb.at[m, r, q], {"tp": 2 * y_at(m) + c},
        )

    def project(q):
        part_ref[:, piece_of(q)] = jnp.dot(
            gated[...], w_ref[:, piece_of(q)], preferred_element_type=F32
        ).astype(BF16)
        for m in range(n_y - 1):
            for r in range(cuts):
                head_pair(m, r, q).start()

    def pair_sum(m, r, q):
        head_pair(m, r, q).wait_recv()
        at, cols = band_of(0, r), piece_of(q)
        tb[m, at, cols] = (
            part_ref[band_of(2 * y_at(m) + c, r), cols].astype(F32) + ra[m, at, cols].astype(F32)
        ).astype(BF16)
        head_far(m, r, q).start()

    def whole_sum(r, q):
        at, cols = band_of(0, r), piece_of(q)
        total = part_ref[band_of(j, r), cols].astype(F32) + ra[n_y - 1, at, cols].astype(F32)
        for m in range(n_y - 1):
            head_far(m, r, q).wait_recv()
            total = total + rb[m, at, cols].astype(F32)
        mixed_ref[at, cols] = total

    def turn_copy(r, i):
        peer = lax.rem(j + 1 + i, n_tp)
        return remote(
            normed.at[band_of(0, r), cols_of(peer)], xcol.at[band_of(j, r)],
            st, vt, {"tp": peer},
        )

    with scope("e_proj"):
        loads[10].wait()
        loop(PARTS, project)
        for r in range(cuts):
            head_near(r).start()
    with scope("e_pair"):
        for r in range(cuts):
            loop((n_y - 1) * PARTS, lambda t: pair_sum(t // PARTS, r, lax.rem(t, PARTS)))
        for copy in loads[11:15]:
            copy.wait()
    for r in range(cuts):
        at = slice(r * band, (r + 1) * band)
        with scope(f"e_rs{r}"):
            head_near(r).wait_recv()
            loop(PARTS, lambda q: whole_sum(r, q))
        with scope(f"e_norm{r}"):
            mid = (
                res_ref[at, :].astype(F32) + rms_scale(mixed_ref[at, :], again_ref[...])
            ).astype(BF16)
            mid_ref[at, :] = mid
            normed[at, :] = rms_scale(mid.astype(F32), bgain_ref[...]).astype(BF16)
        loop(n_tp - 1, lambda i: turn_copy(r, i).start())
        xcol[band_of(j, r), :] = normed[at, cols_of(j)]
    with scope("e_turn"):
        landed(xcol.at[0 : (n_tp - 1) * rows], vt)

    def picked(i):
        return jnp.dot(sel_ref[i], xcol[...], preferred_element_type=F32).astype(BF16)

    def out_copy(i):
        return remote(
            outgoing.at[i], rows_ref.at[i, :, cols_of(j)], ss, vs.at[i],
            {"sp": peer_of(i)},
        )

    def y_copy(i, m):
        place = rows_ref.at[i, :, cols_of(j)]
        return remote(place, place, sy, vy.at[m, i], {"tp": 2 * y_at(m) + c})

    def pair_forward(i, owner):
        place = rows_ref.at[i, :, cols_of(owner)]
        return remote(place, place, sd, vd.at[i], {"tp": sibling})

    def forward(i):
        for m in range(n_y - 1):
            y_copy(i, m).start()
        pair_forward(i, j).start()

    def arrived(i):
        out_copy(i).wait_recv()
        forward(i)

    def relay(i):
        for m in range(n_y - 1):
            y_copy(i, m).wait_recv()
            pair_forward(i, 2 * y_from(m) + c).start()

    def ready(i):
        landed(rows_ref.at[i, :, 0 : n_y * share], vd.at[i])

    def part_pair(i, m):
        return remote(
            p_ref.at[i, :, cols_of(2 * y_at(m) + 1 - c)], r1.at[i, m],
            s1, v1.at[i, m], {"tp": sibling},
        )

    def part_far(i, m):
        return remote(
            ty.at[i, m], r2.at[i, m], s2, v2.at[i, m], {"tp": 2 * y_at(m) + c}
        )

    def back_copy(i, h):
        slot = i if h == 0 else jnp.where(i == n_sp - 1, n_sp, i)
        return remote(ob.at[h, i], back.at[h, i], s3, v3.at[slot], {"sp": peer_of(i)})

    def pass_along(i):
        for m in range(n_y - 1):
            part_pair(i, m).wait_recv()
            ty[i, m] = (
                p_ref[i, :, cols_of(2 * y_at(m) + c)].astype(F32) + r1[i, m].astype(F32)
            ).astype(BF16)
            part_far(i, m).start()

    def summed(i):
        part_pair(i, n_y - 1).wait_recv()
        total = p_ref[i, :, cols_of(j)].astype(F32) + r1[i, n_y - 1].astype(F32)
        for m in range(n_y - 1):
            part_far(i, m).wait_recv()
            total = total + r2[i, m].astype(F32)
        return total.astype(BF16)

    def give_back(i):
        total = summed(i)
        for h in range(2):
            if isinstance(i, int) and i == 0:
                back[h, 0] = total[:, h * narrow : (h + 1) * narrow]
            else:
                ob[h, i] = total[:, h * narrow : (h + 1) * narrow]
                back_copy(i, h).start()

    narrow = share // 2
    tile = min(TILE, wg.shape[1])
    steps = wg.shape[1] // tile

    def run_expert(first, count, after_first, after_up, after_first_down):
        batch = count * cap

        for t in range(steps):
            cols = slice(t * tile, (t + 1) * tile)
            fed = rows_ref[pl.ds(first, count)].reshape(batch, model)
            gate = jnp.dot(fed, wg[:, cols], preferred_element_type=F32)
            rise = jnp.dot(fed, wu[:, cols], preferred_element_type=F32)
            hidden[0:batch, cols] = (gate * jax.nn.sigmoid(gate) * rise).astype(BF16)

            if t == 0:
                after_first()
        after_up()

        def down(m):
            cols = pl.ds(pl.multiple_of(2 * y_at(m) * share, 2 * share), 2 * share)
            made = jnp.dot(hidden[0:batch, :], wd[:, cols], preferred_element_type=F32)
            p_ref[pl.ds(first, count), :, cols] = made.astype(BF16).reshape(
                count, cap, 2 * share
            )
            for i in range(count):
                part_pair(first + i, m).start()

            @pl.when(m == 0)
            def _():
                after_first_down()

        loop(n_y, down)

    inner = (4 * pair >= n_pair) & (4 * pair < 3 * n_pair)
    spare = [(i, 2) for i in range(2, half, 2)]
    units = (
        [(0, 2), (half, 1), (half + 1, 1)] + spare + [(i, 1) for i in range(half + 2, n_sp)]
    )
    total_units = len(units)
    acts = {"arr": arrived, "relay": relay, "ready": ready, "pass": pass_along, "give": give_back}
    hooks = schedule(half, len(spare))

    def act(name, k):
        first, count = units[k]
        for i in range(count):
            if name == "arr" and k == 0 and i == 0:
                continue
            with scope(f"w_{name}{k}{i}"):
                acts[name](first + i)

    def fire(k, slot):
        for name, other in hooks.get((k, slot), ()):
            act(name, other)

    with scope("e_send"):
        rows_ref[0, :, cols_of(j)] = picked(0)
        forward(0)

        def send(t):
            lead = half // 2
            far_first = jnp.where(
                t < lead, half + t, jnp.where(t < lead + half - 1, t - lead + 1, t + 1)
            )
            i = jnp.where(inner, t + 1, far_first)
            outgoing[i] = picked(i)
            out_copy(i).start()

        loop(n_sp - 1, send)
    with scope("e_arrive"):
        act("arr", 0)
        relay(0)
        arrived(2)
        act("arr", 1)
    with scope("e_relay"):
        relay(1)
        for i in range(3, half):
            with scope(f"w_near{i}"):
                arrived(i)
    with scope("e_weights"):
        for copy in loads[15:]:
            copy.wait()
    for k, (first, count) in enumerate(units):
        with scope(f"e_ready{k}"):
            act("ready", k)
        with scope(f"e_run{k}"):
            run_expert(
                first, count, lambda: fire(k, "first"), lambda: fire(k, "up"),
                lambda: fire(k, "down"),
            )
    with scope("e_give"):
        fire(total_units, "first")

    def weighed(i, h):
        return contract(mix_ref[i], back[h, i], 0, 0)

    def home_copy(h, i):
        peer = lax.rem(j + 1 + i, n_tp)
        return remote(
            branch.at[h, rows_of(peer)], brow.at[j, h], s4, v4, {"tp": peer}
        )

    with scope("e_gather"):
        for h in range(2):
            acc[h] = weighed(0, h)

        def gather(i):
            with scope("w_back"):
                landed(back.at[:, i], v3.at[i])
            for h in range(2):
                acc[h] = acc[h] + weighed(i, h)

        loop(half - 1, lambda t: gather(half + t))
        loop(half - 1, lambda t: gather(1 + t))
        for h in range(2):
            back_copy(n_sp - 1, h).wait_recv()
            branch[h] = (acc[h] + weighed(n_sp - 1, h)).astype(BF16)
            loop(n_tp - 1, lambda i: home_copy(h, i).start())
            brow[j, h] = branch[h, rows_of(j), :]

    with scope("e_drain"):
        pair_copy.wait_send()
        exch_copy.wait_send()

        def drain_z(i):
            @pl.when(n_pair - 1 - i > pair)
            def _():
                z_copy(i).wait_send()

        loop(n_pair - 1, drain_z)
        left(part_ref.at[0 : n_y * rows], sa)
        left(tb.at[0 : n_y - 1], sb)
        left(normed.at[:, 0 : (n_tp - 1) * share], st)
        left(outgoing.at[1:n_sp], ss)
        left(rows_ref.at[:, :, 0 : (n_y - 1) * share], sy)
        left(rows_ref.at[:, :, 0 : n_y * share], sd)
        left(p_ref.at[:, :, 0 : n_y * share], s1)
        left(p_ref.at[:, :, 0 : (n_y - 1) * share], s2)
        left(ob.at[:, 1:n_sp], s3)
    with scope("e_home"):
        landed(brow.at[0 : n_tp - 1], v4)
    with scope("e_out"):
        places = [(s, h) for s in range(n_tp) for h in range(2)]
        square = sum(
            jnp.sum(brow[s, h].astype(F32) * brow[s, h].astype(F32), axis=-1, keepdims=True)
            for s, h in places
        )
        scale = lax.rsqrt(square * (1.0 / model) + EPSILON)
        for s, h in places:
            cols = slice(s * share + h * narrow, s * share + (h + 1) * narrow)
            out_ref[:, cols] = (
                mid_ref[:, cols].astype(F32) + brow[s, h].astype(F32) * scale * fgain_ref[:, cols]
            ).astype(BF16)
        left(branch.at[:, 0 : (n_tp - 1) * rows], s4)


def dmas(*shapes):
    return [pltpu.SemaphoreType.DMA(s) for s in shapes]


def shards(
    n_sp,
    n_tp,
    query_matrix,
    key_matrix,
    value_matrix,
    output_gate_rows,
    decay_preactivation,
    channel_decay_bias,
    extra_log_decay,
    head_norm_gain,
    output_projection,
    residual_input,
    attention_norm_gain,
    expert_before_gain,
    expert_after_gain,
    expert_gate_weight,
    expert_up_weight,
    expert_down_weight,
    token_expert_index,
    routing_weight_matrix,
):
    length, width = query_matrix.shape
    model = output_projection.shape[1]
    rows = residual_input.shape[0]
    share = model // n_tp
    n_y = n_tp // 2
    capacity = 5 * length // (2 * n_sp)
    cap = (capacity + 15) // 16 * 16
    values = value_matrix.shape[1]
    hidden_units = expert_gate_weight.shape[2]
    by_peer = (n_sp, n_y)
    state = (DV + FADE_ROWS, width // 2)

    operands = (
        decay_preactivation,
        channel_decay_bias.reshape(1, width),
        extra_log_decay.T,
        key_matrix,
        value_matrix,
        query_matrix,
        output_gate_rows,
        head_norm_gain.reshape(1, DV),
        token_expert_index.T,
        routing_weight_matrix.T,
        output_projection,
        residual_input,
        attention_norm_gain.reshape(1, model),
        expert_before_gain.reshape(1, model),
        expert_after_gain.reshape(1, model),
        expert_gate_weight[0],
        expert_up_weight[0],
        expert_down_weight[0],
    )
    kept = [pltpu.VMEM(a.shape, a.dtype) for a in operands]
    return pl.pallas_call(
        functools.partial(layer_kernel, n_sp, n_tp, cap),
        out_shape=jax.ShapeDtypeStruct((rows, model), BF16),
        in_specs=[pl.BlockSpec(memory_space=pl.ANY)] * len(operands),
        out_specs=pl.BlockSpec(memory_space=pltpu.VMEM),
        scratch_shapes=kept
        + [
            pltpu.VMEM((2,) + state, BF16),
            pltpu.VMEM(state, BF16),
            pltpu.VMEM(state, BF16),
            pltpu.VMEM((n_sp // 2,) + state, BF16),
            pltpu.VMEM((DV, width // 2), F32),
            pltpu.VMEM((DV, width // 2), BF16),
            pltpu.VMEM((DV, width // 2), BF16),
            pltpu.VMEM((length, values), BF16),
            pltpu.VMEM((length, model), BF16),
            pltpu.VMEM((rows, model), F32),
            pltpu.VMEM((n_y, rows, model), BF16),
            pltpu.VMEM((n_y, rows, model), BF16),
            pltpu.VMEM((n_y, rows, model), BF16),
            pltpu.VMEM((rows, model), BF16),
            pltpu.VMEM((length, share), BF16),
            pltpu.VMEM((n_sp, cap, length), BF16),
            pltpu.VMEM((n_sp, cap, length), BF16),
            pltpu.VMEM((n_sp, cap, share), BF16),
            pltpu.VMEM((n_sp, cap, model), BF16),
            pltpu.VMEM((2 * cap, hidden_units), BF16),
            pltpu.VMEM((n_sp, cap, model), BF16),
            pltpu.VMEM(by_peer + (cap, share), BF16),
            pltpu.VMEM(by_peer + (cap, share), BF16),
            pltpu.VMEM(by_peer + (cap, share), BF16),
            pltpu.VMEM((2, n_sp, cap, share // 2), BF16),
            pltpu.VMEM((2, n_sp, cap, share // 2), BF16),
            pltpu.VMEM((2, length, share // 2), F32),
            pltpu.VMEM((2, length, share // 2), BF16),
            pltpu.VMEM((n_tp, 2, rows, share // 2), BF16),
            pltpu.VMEM((rows, model), BF16),
        ]
        + dmas(
            (len(operands),), (2,), (2,), (n_sp // 2,), (n_sp // 2,),
            (), (n_y - 1, 2, PARTS), (2,), (), (n_y - 1, 2, PARTS), (), (), (), (n_sp,),
            (), (n_y - 1, n_sp), (), (n_sp,), (), by_peer, (), by_peer,
            (), (n_sp + 1,), (), (),
        ),
        compiler_params=pltpu.CompilerParams(
            collective_id=1, has_side_effects=True, vmem_limit_bytes=VMEM_LIMIT
        ),
    )(*operands)


def solution(mesh):
    placed = (
        P("sp", "tp"),
        P("sp", "tp"),
        P("sp", "tp"),
        P("sp", "tp"),
        P("sp", "tp"),
        P("tp"),
        P("sp", "tp"),
        P(),
        P("tp", None),
        P(("sp", "tp"), None),
        P(),
        P(),
        P(),
        P("sp", None, "tp"),
        P("sp", None, "tp"),
        P("sp", "tp", None),
        P("sp", None),
        P("sp", None),
    )
    return jax.shard_map(
        functools.partial(shards, mesh.shape["sp"], mesh.shape["tp"]),
        mesh=mesh,
        in_specs=placed,
        out_specs=P(("sp", "tp"), None),
        check_vma=False,
    )
```

```python
import contextlib
import functools

import jax
import jax.numpy as jnp
from jax import lax
from jax.experimental import pallas as pl
from jax.experimental.pallas import tpu as pltpu
from jax.sharding import PartitionSpec as P

KEY_CHANNELS = 64
DV = 128
TOP = 2
BLOCK = 64

EPSILON = 1e-06
DECAY_NORMALIZER = 16.0
HIGHEST = lax.Precision.HIGHEST
MESH = pl.DeviceIdType.MESH
F32 = jnp.float32
BF16 = jnp.bfloat16
FADE_ROWS = 16
PARTS = 4
TILE = 1024
VMEM_LIMIT = 67043328


def scope(name):
    return contextlib.nullcontext()


def rms_scale(values, gain_row):
    return (
        values * lax.rsqrt(jnp.mean(values * values, axis=-1, keepdims=True) + EPSILON) * gain_row
    )


def contract(a, b, da, db):
    return lax.dot_general(a, b, (((da,), (db,)), ((), ())), preferred_element_type=F32)


def loop(count, body):
    def step(i, carry):
        body(i)
        return carry

    lax.fori_loop(0, count, step, 0)


def remote(src, dst, send, recv, device):
    return pltpu.make_async_remote_copy(
        src_ref=src,
        dst_ref=dst,
        send_sem=send,
        recv_sem=recv,
        device_id=device,
        device_id_type=MESH,
    )


def flipped(me, i, n):
    total, bit = 0, 1
    while bit < n:
        total = total + lax.rem(me // bit + i // bit, 2) * bit
        bit *= 2
    return total


def thirds(values):
    high = values.astype(BF16)
    rest = values - high.astype(F32)
    mid = rest.astype(BF16)
    return high, mid, (rest - mid.astype(F32)).astype(BF16)


def schedule(far, spare):
    hooks = {}
    start = 0
    near = list(range(3, 3 + spare))
    units = [1, 2] + list(range(3 + spare, 1 + spare + far))
    end = 1 + spare + far

    def put(k, slot, name, unit):
        hooks.setdefault((k, slot), []).append((name, unit))

    put(start, "up", "relay", units[0])
    for k in near[1:]:
        put(start, "down", "arr", k)
    put(units[0], "up", "relay", units[1])
    put(units[0], "down", "arr", units[2])
    put(units[1], "first", "pass", units[0])
    put(units[1], "up", "arr", units[3])
    for k in near:
        put(k - 1, "up", "relay", k)
    put(near[0], "first", "pass", units[1])
    put(near[0], "first", "pass", start)
    put(near[-1], "up", "relay", units[2])
    put(near[-1], "down", "give", units[0])
    for t in range(2, far):
        if t > 2:
            put(units[t], "first", "give", units[t - 2])
            put(units[t], "first", "pass", units[t - 1])
        if t + 1 < far:
            put(units[t], "up", "relay", units[t + 1])
        if t + 2 < far:
            put(units[t], "down", "arr", units[t + 2])
    put(end, "first", "pass", units[-1])
    for k in near:
        put(end, "first", "pass", k)
    put(end, "first", "give", units[-2])
    put(end, "first", "give", start)
    put(end, "first", "give", units[-1])
    for k in near:
        put(end, "first", "give", k)
    return hooks


def layer_kernel(
    n_sp, n_tp, cap,
    d_hbm, bias_hbm, extra_hbm, k_hbm, v_hbm, q_hbm, g_hbm, hgain_hbm, index_hbm, weight_hbm,
    w_hbm, res_hbm, again_hbm, bgain_hbm, fgain_hbm, wg_hbm, wu_hbm, wd_hbm,
    out_ref,
    d_ref, bias_ref, extra_ref, k_ref, v_ref, q_ref, g_ref, hgain_ref, index_ref, weight_ref,
    w_ref, res_ref, again_ref, bgain_ref, fgain_ref, wg, wu, wd,
    message, pairbox, zmsg, inbox, carried, exch_out, exch_in, gated, part_ref, mixed_ref,
    ra, rb, tb, normed, xcol, sel_ref, mix_ref, outgoing, rows_ref, hidden, p_ref,
    r1, r2, ty, ob, back, acc, branch, brow, mid_ref,
    load, s_pair, r_pair, s_z, r_z,
    sa, va, vn, sb, vb, st, vt, ss, vs, sy, vy, sd, vd, s1, v1, s2, v2, s3, v3, s4, v4,
):
    me = lax.axis_index("sp")
    j = lax.axis_index("tp")
    loads = [
        pltpu.make_async_copy(src, dst, load.at[n])
        for n, (src, dst) in enumerate(
            (
                (d_hbm, d_ref),
                (bias_hbm, bias_ref),
                (extra_hbm, extra_ref),
                (k_hbm, k_ref),
                (v_hbm, v_ref),
                (q_hbm, q_ref),
                (g_hbm, g_ref),
                (hgain_hbm, hgain_ref),
                (index_hbm, index_ref),
                (weight_hbm, weight_ref),
                (w_hbm, w_ref),
                (res_hbm, res_ref),
                (again_hbm, again_ref),
                (bgain_hbm, bgain_ref),
                (fgain_hbm, fgain_ref),
                (wg_hbm, wg),
                (wu_hbm, wu),
                (wd_hbm, wd),
            )
        )
    ]
    for copy in loads:
        copy.start()
    barrier = pltpu.get_barrier_semaphore()

    def along_sp(i):
        pl.semaphore_signal(
            barrier, inc=1, device_id={"sp": lax.rem(me + 1 + i, n_sp)}, device_id_type=MESH
        )

    def along_tp(i):
        pl.semaphore_signal(
            barrier, inc=1, device_id={"tp": lax.rem(j + 1 + i, n_tp)}, device_id_type=MESH
        )

    loop(n_sp - 1, along_sp)
    loop(n_tp - 1, along_tp)

    side = lax.rem(me, 2)
    pair = me // 2
    n_pair = n_sp // 2
    partner = me + 1 - 2 * side
    n_y = n_tp // 2
    y, c = j // 2, lax.rem(j, 2)
    sibling = 2 * y + 1 - c
    length, width = q_ref.shape
    rows, model = res_ref.shape
    share = model // n_tp
    half = n_sp // 2
    heads = width // KEY_CHANNELS
    blocks = length // BLOCK
    half_width = width // 2

    with scope("a_wait0"):
        for copy in loads[0:3]:
            copy.wait()
    with scope("a_decay"):
        x = d_ref[...].astype(F32) + bias_ref[...]
        log_decay = (jnp.minimum(x, 0.0) - jnp.log1p(jnp.exp(-jnp.abs(x)))) / DECAY_NORMALIZER
        row = lax.broadcasted_iota(jnp.int32, (length, length), 0)
        col = lax.broadcasted_iota(jnp.int32, (length, length), 1)
        causal = (row >= col) & (row // BLOCK == col // BLOCK)
        triangle = jnp.where(causal, 1.0, 0.0).astype(F32)
        ones = triangle.astype(BF16)
        inside = sum(jnp.dot(ones, p, preferred_element_type=F32) for p in thirds(log_decay))
        extra = lax.dot_general(
            triangle, extra_ref[...], (((1,), (1,)), ((), ())), precision=HIGHEST,
            preferred_element_type=F32,
        )
        inside = inside + jnp.concatenate(
            [jnp.broadcast_to(extra[:, h : h + 1], (length, KEY_CHANNELS)) for h in range(heads)],
            axis=1,
        )
    ends = [inside[(b + 1) * BLOCK - 1 : (b + 1) * BLOCK, :] for b in range(blocks)]
    offsets = [jnp.zeros_like(ends[0])]
    for b in range(blocks):
        offsets.append(offsets[-1] + ends[b])

    def spread(pieces):
        return jnp.concatenate([jnp.broadcast_to(r, (BLOCK, width)) for r in pieces], axis=0)

    for copy in loads[3:6]:
        copy.wait()
    with scope("a_state"):
        q = q_ref[...].astype(F32) * KEY_CHANNELS ** (-0.5)
        k = k_ref[...].astype(F32)
        k_end = (k * jnp.exp(spread(ends) - inside)).astype(BF16)
        states = [jnp.zeros((DV, width), F32)]
        for b in range(blocks):
            at = slice(b * BLOCK, (b + 1) * BLOCK)
            grown = jnp.concatenate(
                [
                    contract(
                        v_ref[at, h * DV : (h + 1) * DV],
                        k_end[at, h * KEY_CHANNELS : (h + 1) * KEY_CHANNELS],
                        0,
                        0,
                    )
                    for h in range(heads)
                ],
                axis=1,
            )
            states.append(states[-1] * jnp.exp(ends[b]) + grown)
        fade = jnp.exp(offsets[-1])
        for h in range(2):
            cs = slice(h * half_width, (h + 1) * half_width)
            message[h, 0:DV, :] = states[-1][:, cs].astype(BF16)
            message[h, DV:, :] = jnp.broadcast_to(fade[:, cs], (FADE_ROWS, half_width)).astype(BF16)

    with scope("a_barrier"):
        pl.semaphore_wait(barrier, n_sp + n_tp - 2)
    pair_copy = remote(
        message.at[1 - side], pairbox, s_pair.at[0], r_pair.at[0], {"sp": partner}
    )
    pair_copy.start()

    with scope("a_local"):
        q_in = (q * jnp.exp(inside)).astype(BF16)
        k_inv = (k * jnp.exp(-inside)).astype(BF16)
        q_all = (q * jnp.exp(inside + spread(offsets[:-1]))).astype(BF16)
        local = []
        for h in range(heads):
            cs = slice(h * KEY_CHANNELS, (h + 1) * KEY_CHANNELS)
            own = jnp.sum(q[:, cs] * k[:, cs], axis=1, keepdims=True)
            scores = jnp.where(causal, contract(q_in[:, cs], k_inv[:, cs], 1, 1), 0.0)
            scores = jnp.where(row == col, own, scores).astype(BF16)
            within = jnp.dot(scores, v_ref[:, h * DV : (h + 1) * DV], preferred_element_type=F32)
            across = jnp.concatenate(
                [jnp.zeros((BLOCK, DV), F32)]
                + [
                    contract(
                        q_in[b * BLOCK : (b + 1) * BLOCK, cs], states[b][:, cs].astype(BF16), 1, 1
                    )
                    for b in range(1, blocks)
                ],
                axis=0,
            )
            local.append(within + across)

    def peer_of(i):
        return flipped(me, i, n_sp)

    with scope("a_route"):
        loads[8].wait()
        loads[9].wait()
        e0, e1 = index_ref[0:1, :], index_ref[1:2, :]
        named = lax.broadcasted_iota(jnp.int32, (n_sp, length), 0)
        taken = jnp.where((named == e0) | (named == e1), 1.0, 0.0).astype(BF16)
        before = jnp.where(row < col, 1.0, 0.0).astype(BF16)
        counts = jnp.dot(taken, before, preferred_element_type=F32)

        def target(e):
            place = jnp.sum(jnp.where(named == e, counts, 0.0), axis=0, keepdims=True)
            return e.astype(F32) * cap + place

        t0, t1 = target(e0), target(e1)
        w0, w1 = weight_ref[0:1, :], weight_ref[1:2, :]

        def route(i):
            slot = lax.broadcasted_iota(jnp.int32, (cap, length), 0) + peer_of(i) * cap
            slot = slot.astype(F32)
            is0, is1 = slot == t0, slot == t1
            sel_ref[i] = jnp.where(is0 | is1, 1.0, 0.0).astype(BF16)
            mix_ref[i] = (jnp.where(is0, w0, 0.0) + jnp.where(is1, w1, 0.0)).astype(BF16)

        loop(n_sp, route)

    with scope("a_pair"):
        pair_copy.wait_recv()
        mine = message[side].astype(F32)
        other = pairbox[...].astype(F32)
        first = jnp.where(side == 0, mine, other)
        second = jnp.where(side == 0, other, mine)
        zmsg[0:DV, :] = (first[0:DV] * second[DV : DV + 1] + second[0:DV]).astype(BF16)
        zmsg[DV:, :] = (first[DV:] * second[DV:]).astype(BF16)

    def z_copy(i):
        return remote(
            zmsg, inbox.at[pair], s_z.at[i], r_z.at[pair],
            {"sp": 2 * (n_pair - 1 - i) + side},
        )

    def z_send(i):
        @pl.when(n_pair - 1 - i > pair)
        def _():
            z_copy(i).start()

    loop(n_pair - 1, z_send)

    carried[...] = jnp.zeros_like(carried)

    def take(hop):
        @pl.when(hop < pair)
        def _():
            remote(
                zmsg, inbox.at[hop], s_z.at[0], r_z.at[hop], {"sp": partner}
            ).wait_recv()
            carried[...] = carried[...] * inbox[hop, DV : DV + 1, :].astype(F32) + inbox[
                hop, 0:DV, :
            ].astype(F32)

    with scope("a_take"):
        loop(n_pair - 1, take)

    with scope("a_exch"):
        before_pair = carried[...]
        head = jnp.where(
            side == 0, message[side].astype(F32), pairbox[...].astype(F32)
        )
        after_first = before_pair * head[DV : DV + 1] + head[0:DV]
        own_start = jnp.where(side == 0, before_pair, after_first)
        exch_out[...] = jnp.where(side == 0, after_first, before_pair).astype(BF16)
        exch_copy = remote(exch_out, exch_in, s_pair.at[1], r_pair.at[1], {"sp": partner})
        exch_copy.start()
        exch_copy.wait_recv()
        got = exch_in[...].astype(F32)
        start = jnp.concatenate(
            [jnp.where(side == 0, own_start, got), jnp.where(side == 0, got, own_start)], axis=1
        ).astype(BF16)

    for copy in loads[6:8]:
        copy.wait()
    with scope("a_gate"):
        for h in range(heads):
            cs = slice(h * KEY_CHANNELS, (h + 1) * KEY_CHANNELS)
            at = slice(h * DV, (h + 1) * DV)
            attn = local[h] + contract(q_all[:, cs], start[:, cs], 1, 1)
            gate = g_ref[:, at].astype(F32)
            gated[:, at] = (rms_scale(attn, hgain_ref[...]) * (gate * jax.nn.sigmoid(gate))).astype(
                BF16
            )

    def landed(ref, sem):
        remote(ref, ref, sem, sem, {"sp": partner}).wait_recv()

    def left(ref, sem):
        remote(ref, ref, sem, sem, {"sp": partner}).wait_send()

    def rows_of(index):
        return pl.ds(pl.multiple_of(index * rows, rows), rows)

    def cols_of(index):
        return pl.ds(pl.multiple_of(index * share, share), share)

    piece = model // PARTS

    def piece_of(q):
        return pl.ds(pl.multiple_of(q * piece, piece), piece)

    def y_at(i):
        return lax.rem(y + 1 + i, n_y)

    def y_from(i):
        return lax.rem(y + n_y - 1 - i, n_y)

    cuts = 2 if rows % 32 == 0 else 1
    band = rows // cuts

    def band_of(index, r):
        return pl.ds(pl.multiple_of(index * rows + r * band, band), band)

    def head_pair(m, r, q):
        return remote(
            part_ref.at[band_of(2 * y_at(m) + 1 - c, r), piece_of(q)],
            ra.at[m, band_of(0, r), piece_of(q)],
            sa, va.at[m, r, q], {"tp": sibling},
        )

    def head_near(r):
        return remote(
            part_ref.at[band_of(sibling, r)], ra.at[n_y - 1, band_of(0, r)], sa, vn.at[r],
            {"tp": sibling},
        )

    def head_far(m, r, q):
        return remote(
            tb.at[m, band_of(0, r), piece_of(q)], rb.at[m, band_of(0, r), piece_of(q)],
            sb, vb.at[m, r, q], {"tp": 2 * y_at(m) + c},
        )

    def project(q):
        part_ref[:, piece_of(q)] = jnp.dot(
            gated[...], w_ref[:, piece_of(q)], preferred_element_type=F32
        ).astype(BF16)
        for m in range(n_y - 1):
            for r in range(cuts):
                head_pair(m, r, q).start()

    def pair_sum(m, r, q):
        head_pair(m, r, q).wait_recv()
        at, cols = band_of(0, r), piece_of(q)
        tb[m, at, cols] = (
            part_ref[band_of(2 * y_at(m) + c, r), cols].astype(F32) + ra[m, at, cols].astype(F32)
        ).astype(BF16)
        head_far(m, r, q).start()

    def whole_sum(r, q):
        at, cols = band_of(0, r), piece_of(q)
        total = part_ref[band_of(j, r), cols].astype(F32) + ra[n_y - 1, at, cols].astype(F32)
        for m in range(n_y - 1):
            head_far(m, r, q).wait_recv()
            total = total + rb[m, at, cols].astype(F32)
        mixed_ref[at, cols] = total

    def turn_copy(r, i):
        peer = lax.rem(j + 1 + i, n_tp)
        return remote(
            normed.at[band_of(0, r), cols_of(peer)], xcol.at[band_of(j, r)],
            st, vt, {"tp": peer},
        )

    with scope("e_proj"):
        loads[10].wait()
        loop(PARTS, project)
        for r in range(cuts):
            head_near(r).start()
    with scope("e_pair"):
        for r in range(cuts):
            loop((n_y - 1) * PARTS, lambda t: pair_sum(t // PARTS, r, lax.rem(t, PARTS)))
        for copy in loads[11:15]:
            copy.wait()
    for r in range(cuts):
        at = slice(r * band, (r + 1) * band)
        with scope(f"e_rs{r}"):
            head_near(r).wait_recv()
            loop(PARTS, lambda q: whole_sum(r, q))
        with scope(f"e_norm{r}"):
            mid = (
                res_ref[at, :].astype(F32) + rms_scale(mixed_ref[at, :], again_ref[...])
            ).astype(BF16)
            mid_ref[at, :] = mid
            normed[at, :] = rms_scale(mid.astype(F32), bgain_ref[...]).astype(BF16)
        loop(n_tp - 1, lambda i: turn_copy(r, i).start())
        xcol[band_of(j, r), :] = normed[at, cols_of(j)]
    with scope("e_turn"):
        landed(xcol.at[0 : (n_tp - 1) * rows], vt)

    def picked(i):
        return jnp.dot(sel_ref[i], xcol[...], preferred_element_type=F32).astype(BF16)

    def out_copy(i):
        return remote(
            outgoing.at[i], rows_ref.at[i, :, cols_of(j)], ss, vs.at[i],
            {"sp": peer_of(i)},
        )

    def y_copy(i, m):
        place = rows_ref.at[i, :, cols_of(j)]
        return remote(place, place, sy, vy.at[m, i], {"tp": 2 * y_at(m) + c})

    def pair_forward(i, owner):
        place = rows_ref.at[i, :, cols_of(owner)]
        return remote(place, place, sd, vd.at[i], {"tp": sibling})

    def forward(i):
        for m in range(n_y - 1):
            y_copy(i, m).start()
        pair_forward(i, j).start()

    def arrived(i):
        out_copy(i).wait_recv()
        forward(i)

    def relay(i):
        for m in range(n_y - 1):
            y_copy(i, m).wait_recv()
            pair_forward(i, 2 * y_from(m) + c).start()

    def ready(i):
        landed(rows_ref.at[i, :, 0 : n_y * share], vd.at[i])

    def part_pair(i, m):
        return remote(
            p_ref.at[i, :, cols_of(2 * y_at(m) + 1 - c)], r1.at[i, m],
            s1, v1.at[i, m], {"tp": sibling},
        )

    def part_far(i, m):
        return remote(
            ty.at[i, m], r2.at[i, m], s2, v2.at[i, m], {"tp": 2 * y_at(m) + c}
        )

    def back_copy(i, h):
        slot = i if h == 0 else jnp.where(i == n_sp - 1, n_sp, i)
        return remote(ob.at[h, i], back.at[h, i], s3, v3.at[slot], {"sp": peer_of(i)})

    def pass_along(i):
        for m in range(n_y - 1):
            part_pair(i, m).wait_recv()
            ty[i, m] = (
                p_ref[i, :, cols_of(2 * y_at(m) + c)].astype(F32) + r1[i, m].astype(F32)
            ).astype(BF16)
            part_far(i, m).start()

    def summed(i):
        part_pair(i, n_y - 1).wait_recv()
        total = p_ref[i, :, cols_of(j)].astype(F32) + r1[i, n_y - 1].astype(F32)
        for m in range(n_y - 1):
            part_far(i, m).wait_recv()
            total = total + r2[i, m].astype(F32)
        return total.astype(BF16)

    def give_back(i):
        total = summed(i)
        for h in range(2):
            if isinstance(i, int) and i == 0:
                back[h, 0] = total[:, h * narrow : (h + 1) * narrow]
            else:
                ob[h, i] = total[:, h * narrow : (h + 1) * narrow]
                back_copy(i, h).start()

    narrow = share // 2
    def run_expert(first, count, last, after_first, after_up, after_first_down):
        batch = count * cap
        tile = min(TILE // 2 if last else TILE, wg.shape[1])
        steps = wg.shape[1] // tile

        for t in range(steps):
            cols = slice(t * tile, (t + 1) * tile)
            fed = rows_ref[pl.ds(first, count)].reshape(batch, model)
            gate = jnp.dot(fed, wg[:, cols], preferred_element_type=F32)
            rise = jnp.dot(fed, wu[:, cols], preferred_element_type=F32)
            hidden[0:batch, cols] = (gate * jax.nn.sigmoid(gate) * rise).astype(BF16)

            if t == 0:
                after_first()
        after_up()

        def down(m):
            cols = pl.ds(pl.multiple_of(2 * y_at(m) * share, 2 * share), 2 * share)
            made = jnp.dot(hidden[0:batch, :], wd[:, cols], preferred_element_type=F32)
            p_ref[pl.ds(first, count), :, cols] = made.astype(BF16).reshape(
                count, cap, 2 * share
            )
            for i in range(count):
                part_pair(first + i, m).start()

            @pl.when(m == 0)
            def _():
                after_first_down()

        loop(n_y, down)

    inner = (4 * pair >= n_pair) & (4 * pair < 3 * n_pair)
    spare = [(i, 2) for i in range(2, half, 2)]
    units = (
        [(0, 2), (half, 1), (half + 1, 1)] + spare + [(i, 1) for i in range(half + 2, n_sp)]
    )
    total_units = len(units)
    acts = {"arr": arrived, "relay": relay, "ready": ready, "pass": pass_along, "give": give_back}
    hooks = schedule(half, len(spare))

    def act(name, k):
        first, count = units[k]
        for i in range(count):
            if name == "arr" and k == 0 and i == 0:
                continue
            with scope(f"w_{name}{k}{i}"):
                acts[name](first + i)

    def second_poll():
        with scope("w_poll2"):
            arrived(jnp.where(top, 2, half + 1))

    def third_poll():
        with scope("w_poll3"):
            arrived(3)

    def fire(k, slot):
        if k == 0 and slot == "first":
            second_poll()
        if k == 0 and slot == "down":
            third_poll()
        for name, other in hooks.get((k, slot), ()):
            act(name, other)

    with scope("e_send"):
        rows_ref[0, :, cols_of(j)] = picked(0)
        forward(0)

        def send(t):
            lead = half // 2
            far_first = jnp.where(
                t < lead, half + t, jnp.where(t < lead + half - 1, t - lead + 1, t + 1)
            )
            i = jnp.where(inner, t + 1, far_first)
            outgoing[i] = picked(i)
            out_copy(i).start()

        loop(n_sp - 1, send)
    with scope("e_arrive"):
        act("arr", 0)
        relay(0)
        act("arr", 1)
    with scope("e_relay"):
        relay(1)
        top = pair == n_pair - 1
        arrived(jnp.where(top, half + 1, 2))
    with scope("e_weights"):
        for copy in loads[15:]:
            copy.wait()
    for k, (first, count) in enumerate(units):
        with scope(f"e_ready{k}"):
            act("ready", k)
        with scope(f"e_run{k}"):
            run_expert(
                first, count, k == total_units - 1, lambda: fire(k, "first"),
                lambda: fire(k, "up"), lambda: fire(k, "down"),
            )
    with scope("e_give"):
        fire(total_units, "first")

    def weighed(i, h):
        return contract(mix_ref[i], back[h, i], 0, 0)

    def home_copy(h, i):
        peer = lax.rem(j + 1 + i, n_tp)
        return remote(
            branch.at[h, rows_of(peer)], brow.at[j, h], s4, v4, {"tp": peer}
        )

    with scope("e_gather"):
        for h in range(2):
            acc[h] = weighed(0, h)

        def gather(i):
            with scope("w_back"):
                landed(back.at[:, i], v3.at[i])
            for h in range(2):
                acc[h] = acc[h] + weighed(i, h)

        loop(half - 1, lambda t: gather(half + t))
        loop(half - 1, lambda t: gather(1 + t))
        for h in range(2):
            back_copy(n_sp - 1, h).wait_recv()
            branch[h] = (acc[h] + weighed(n_sp - 1, h)).astype(BF16)
            loop(n_tp - 1, lambda i: home_copy(h, i).start())
            brow[j, h] = branch[h, rows_of(j), :]

    with scope("e_drain"):
        pair_copy.wait_send()
        exch_copy.wait_send()

        def drain_z(i):
            @pl.when(n_pair - 1 - i > pair)
            def _():
                z_copy(i).wait_send()

        loop(n_pair - 1, drain_z)
        left(part_ref.at[0 : n_y * rows], sa)
        left(tb.at[0 : n_y - 1], sb)
        left(normed.at[:, 0 : (n_tp - 1) * share], st)
        left(outgoing.at[1:n_sp], ss)
        left(rows_ref.at[:, :, 0 : (n_y - 1) * share], sy)
        left(rows_ref.at[:, :, 0 : n_y * share], sd)
        left(p_ref.at[:, :, 0 : n_y * share], s1)
        left(p_ref.at[:, :, 0 : (n_y - 1) * share], s2)
        left(ob.at[:, 1:n_sp], s3)
    with scope("e_home"):
        landed(brow.at[0 : n_tp - 1], v4)
    with scope("e_out"):
        places = [(s, h) for s in range(n_tp) for h in range(2)]
        square = sum(
            jnp.sum(brow[s, h].astype(F32) * brow[s, h].astype(F32), axis=-1, keepdims=True)
            for s, h in places
        )
        scale = lax.rsqrt(square * (1.0 / model) + EPSILON)
        for s, h in places:
            cols = slice(s * share + h * narrow, s * share + (h + 1) * narrow)
            out_ref[:, cols] = (
                mid_ref[:, cols].astype(F32) + brow[s, h].astype(F32) * scale * fgain_ref[:, cols]
            ).astype(BF16)
        left(branch.at[:, 0 : (n_tp - 1) * rows], s4)


def dmas(*shapes):
    return [pltpu.SemaphoreType.DMA(s) for s in shapes]


def shards(
    n_sp,
    n_tp,
    query_matrix,
    key_matrix,
    value_matrix,
    output_gate_rows,
    decay_preactivation,
    channel_decay_bias,
    extra_log_decay,
    head_norm_gain,
    output_projection,
    residual_input,
    attention_norm_gain,
    expert_before_gain,
    expert_after_gain,
    expert_gate_weight,
    expert_up_weight,
    expert_down_weight,
    token_expert_index,
    routing_weight_matrix,
):
    length, width = query_matrix.shape
    model = output_projection.shape[1]
    rows = residual_input.shape[0]
    share = model // n_tp
    n_y = n_tp // 2
    capacity = 5 * length // (2 * n_sp)
    cap = (capacity + 15) // 16 * 16
    values = value_matrix.shape[1]
    hidden_units = expert_gate_weight.shape[2]
    by_peer = (n_sp, n_y)
    state = (DV + FADE_ROWS, width // 2)

    operands = (
        decay_preactivation,
        channel_decay_bias.reshape(1, width),
        extra_log_decay.T,
        key_matrix,
        value_matrix,
        query_matrix,
        output_gate_rows,
        head_norm_gain.reshape(1, DV),
        token_expert_index.T,
        routing_weight_matrix.T,
        output_projection,
        residual_input,
        attention_norm_gain.reshape(1, model),
        expert_before_gain.reshape(1, model),
        expert_after_gain.reshape(1, model),
        expert_gate_weight[0],
        expert_up_weight[0],
        expert_down_weight[0],
    )
    kept = [pltpu.VMEM(a.shape, a.dtype) for a in operands]
    return pl.pallas_call(
        functools.partial(layer_kernel, n_sp, n_tp, cap),
        out_shape=jax.ShapeDtypeStruct((rows, model), BF16),
        in_specs=[pl.BlockSpec(memory_space=pl.ANY)] * len(operands),
        out_specs=pl.BlockSpec(memory_space=pltpu.VMEM),
        scratch_shapes=kept
        + [
            pltpu.VMEM((2,) + state, BF16),
            pltpu.VMEM(state, BF16),
            pltpu.VMEM(state, BF16),
            pltpu.VMEM((n_sp // 2,) + state, BF16),
            pltpu.VMEM((DV, width // 2), F32),
            pltpu.VMEM((DV, width // 2), BF16),
            pltpu.VMEM((DV, width // 2), BF16),
            pltpu.VMEM((length, values), BF16),
            pltpu.VMEM((length, model), BF16),
            pltpu.VMEM((rows, model), F32),
            pltpu.VMEM((n_y, rows, model), BF16),
            pltpu.VMEM((n_y, rows, model), BF16),
            pltpu.VMEM((n_y, rows, model), BF16),
            pltpu.VMEM((rows, model), BF16),
            pltpu.VMEM((length, share), BF16),
            pltpu.VMEM((n_sp, cap, length), BF16),
            pltpu.VMEM((n_sp, cap, length), BF16),
            pltpu.VMEM((n_sp, cap, share), BF16),
            pltpu.VMEM((n_sp, cap, model), BF16),
            pltpu.VMEM((2 * cap, hidden_units), BF16),
            pltpu.VMEM((n_sp, cap, model), BF16),
            pltpu.VMEM(by_peer + (cap, share), BF16),
            pltpu.VMEM(by_peer + (cap, share), BF16),
            pltpu.VMEM(by_peer + (cap, share), BF16),
            pltpu.VMEM((2, n_sp, cap, share // 2), BF16),
            pltpu.VMEM((2, n_sp, cap, share // 2), BF16),
            pltpu.VMEM((2, length, share // 2), F32),
            pltpu.VMEM((2, length, share // 2), BF16),
            pltpu.VMEM((n_tp, 2, rows, share // 2), BF16),
            pltpu.VMEM((rows, model), BF16),
        ]
        + dmas(
            (len(operands),), (2,), (2,), (n_sp // 2,), (n_sp // 2,),
            (), (n_y - 1, 2, PARTS), (2,), (), (n_y - 1, 2, PARTS), (), (), (), (n_sp,),
            (), (n_y - 1, n_sp), (), (n_sp,), (), by_peer, (), by_peer,
            (), (n_sp + 1,), (), (),
        ),
        compiler_params=pltpu.CompilerParams(
            collective_id=1, has_side_effects=True, vmem_limit_bytes=VMEM_LIMIT
        ),
    )(*operands)


def solution(mesh):
    placed = (
        P("sp", "tp"),
        P("sp", "tp"),
        P("sp", "tp"),
        P("sp", "tp"),
        P("sp", "tp"),
        P("tp"),
        P("sp", "tp"),
        P(),
        P("tp", None),
        P(("sp", "tp"), None),
        P(),
        P(),
        P(),
        P("sp", None, "tp"),
        P("sp", None, "tp"),
        P("sp", "tp", None),
        P("sp", None),
        P("sp", None),
    )
    return jax.shard_map(
        functools.partial(shards, mesh.shape["sp"], mesh.shape["tp"]),
        mesh=mesh,
        in_specs=placed,
        out_specs=P(("sp", "tp"), None),
        check_vma=False,
    )
```
